32 devices in a mesh: kv: 8 (over z, x), tp: 4 (over y, core).
Axes of the slice: x: 2, y: 2, z: 4, core: 2. Of those that a mesh axis runs over, the one named last changes fastest.
Arguments:
- queries: bfloat16 [1024, 2048], P('kv', 'tp'), may hold values from -6 to 6
- keys: bfloat16 [1024, 2048], P('kv', 'tp'), may hold values from -6 to 6
- values: bfloat16 [1024, 2048], P('kv', 'tp'), may hold values from -6 to 6
- attended: bfloat16 [1024, 2048], P('kv', 'tp'), may hold values from -6 to 6
- cotangent: bfloat16 [1024, 2048], P('kv', 'tp'), may hold values from -96 to 96
- log_totals: float32 [32, 1024], P('tp', 'kv'), may hold values from 4 to 7
- block_picks: int32 [32, 16, 8], P('tp', 'kv'), may hold values from -1 to 14, as said below
- normed: bfloat16 [1024, 4096], P('kv', 'tp'), may hold values from -6 to 6
Outputs:
- grad_queries: bfloat16 [1024, 2048], P('kv', 'tp')
- grad_keys: bfloat16 [1024, 2048], P('kv', 'tp')
- grad_values: bfloat16 [1024, 2048], P('kv', 'tp')
- grad_weight: float32 [4096, 2048], P('kv', 'tp')
The draws below stay inside these ranges and needn't reach their ends.
Inputs may be any that keep to these rules, and one draw needn't show every extreme that they name: `block_picks`: row c of head h names at most 8 distinct blocks below c, followed by -1 in the other slots. One key block is named by at most 4 query blocks of one head, and in every draw each head has a block named exactly 4 times.
All inputs are finite; a program needn't handle non-finite values.
Results may differ from the reference program's by a relative error of at most 0.0069.
Values may be sent and summed in bfloat16 or wider, within the bound.
A program may use at most 128 MiB of HBM per device.

```python
import jax
import jax.numpy as jnp
from jax import lax

D = 4096
H = 32
DH = 64
BLOCK = 64
SEL = 8
TOKENS = 1024
NQB = 16
MOST = 4


def draw_block_picks(key, part):
    key_jitter, key_hot = jax.random.split(jax.random.fold_in(key, 17))
    jitter = jax.random.randint(key_jitter, (H, NQB, NQB), 0, 2 ** 24 // NQB)
    hot_ids = jax.random.randint(key_hot, (H, 3), 0, max(1, NQB // 4))
    block_ids = jnp.arange(NQB)

    def one_head(jitter_h, hot_h):
        others = jnp.any(block_ids[:, None] == hot_h[None, 1:], axis=1)

        def advance(tallies, qblock):
            levels = jnp.where(others, 2, 1)
            levels = jnp.where(block_ids == qblock - NQB // 2, 3, levels)
            levels = jnp.where(block_ids == qblock - 1, 4, levels)
            levels = jnp.where(block_ids == hot_h[0], 5, levels)
            usable = (block_ids < qblock) & (tallies < MOST)
            scores = jnp.where(usable, levels * 2 ** 24 + jitter_h[qblock] * NQB + block_ids, -(block_ids + 1))
            top_vals, chosen_ids = lax.top_k(scores, SEL)
            row_ids = jnp.where(top_vals >= 0, chosen_ids, -1).astype(jnp.int32)
            tallies = tallies + jnp.sum((row_ids[:, None] == block_ids[None, :]).astype(jnp.int32), axis=0)
            return (tallies, row_ids)
        _, table = lax.scan(advance, jnp.zeros((NQB,), jnp.int32), jnp.arange(NQB))
        return table
    return jax.vmap(one_head)(jitter, hot_ids).astype(jnp.int32)


def spiked(entries, key, source, target, parts, factor):
    def block_of(dim):
        return (jnp.arange(entries.shape[dim]) // (entries.shape[dim] // parts)).reshape((-1,) + (1,) * (entries.ndim - 1 - dim))

    one_side = jax.random.permutation(key, parts)[block_of(target)]
    other_side = (block_of(target) + parts // 2) % parts
    return jnp.where((block_of(source) == one_side) | (block_of(source) == other_side), factor * entries, entries)


def block_levels(rng, shape, cuts, smallest, high):
    def one(position, blocks):
        steps = jax.random.uniform(jax.random.fold_in(jax.random.fold_in(rng, 6), position), (blocks,), jnp.float32, smallest / len(cuts), high / len(cuts))
        return jnp.repeat(jnp.exp(steps), shape[position] // blocks).reshape((-1,) + (1,) * (len(shape) - position - 1))

    loudness = one(*cuts[0])
    for cut in cuts[1:]:
        loudness = loudness * one(*cut)
    return loudness


def centred(stream_key, shape, width, most, shards=(), held_as=jnp.bfloat16):
    values = width * jax.random.normal(stream_key, shape, jnp.float32)
    if shards:
        values = values * block_levels(stream_key, shape, shards, -0.22, 0.18)
    return jnp.clip(values, -most, most).astype(held_as)


def heavy_noise(rng, extent, scale, limit, cuts, heavy, kind=jnp.bfloat16):
    result = scale * jax.random.normal(rng, extent, jnp.float32)
    if cuts:
        result = result * block_levels(rng, extent, cuts, -0.22, 0.18)
    return jnp.clip(spiked(result, jax.random.fold_in(rng, 3), *heavy), -limit, limit).astype(kind)


def setup_inputs(seed: int = 0) -> dict:
    splits = jax.random.split(jax.random.key(seed), 9)
    queries = centred(splits[0], (TOKENS, H * DH), 1.0, 6.0, ((0, 8), (1, 4)))
    keys = centred(splits[1], (TOKENS, H * DH), 1.0, 6.0, ((0, 8), (1, 4)))
    values = centred(splits[2], (TOKENS, H * DH), 1.0, 6.0, ((0, 8), (1, 4)))
    attended = centred(splits[3], (TOKENS, H * DH), 1.0, 6.0, ((0, 8), (1, 4)))
    cotangent = centred(splits[4], (TOKENS, H * DH), 16.0, 96.0, ((0, 8), (1, 4)))
    log_totals = jnp.clip(4.0 + 3.0 * jax.random.uniform(splits[5], (H, TOKENS), jnp.float32) ** block_levels(splits[5], (H, TOKENS), ((0, 4), (1, 8)), -0.2, 0.2), 4.0, 7.0)
    block_picks = draw_block_picks(jax.random.fold_in(splits[8], 71), 0)
    normed = heavy_noise(splits[7], (TOKENS, D), 1.0, 6.0, ((0, 8), (1, 4)), (0, 1, 8, 2.0))
    return {"queries": queries, "keys": keys, "values": values, "attended": attended, "cotangent": cotangent, "log_totals": log_totals, "block_picks": block_picks, "normed": normed}


def tile_grads(q_tile, k_tile, v_tile, g_tile, log_total, row_dots, allowed):
    scale = q_tile.shape[-1] ** -0.5
    scores = jnp.einsum('...qd,...kd->...qk', q_tile, k_tile) * scale
    probs = jnp.where(allowed, jnp.exp(scores - log_total[..., None]), 0.0)
    probs_low = lax.optimization_barrier(probs.astype(jnp.bfloat16)).astype(jnp.float32)
    grad_v = jnp.einsum('...qk,...qd->...kd', probs_low, g_tile)
    grad_p = jnp.einsum('...qd,...kd->...qk', g_tile, v_tile)
    grad_s = (probs * (grad_p - row_dots[..., None])).astype(jnp.bfloat16)
    grad_s = lax.optimization_barrier(grad_s).astype(jnp.float32)
    grad_q = jnp.einsum('...qk,...kd->...qd', grad_s, k_tile) * scale
    grad_k = jnp.einsum('...qk,...qd->...kd', grad_s, q_tile) * scale
    return grad_q, grad_k, grad_v


def by_head(matrix):
    return matrix.astype(jnp.float32).reshape(NQB, BLOCK, H, DH).transpose(2, 0, 1, 3)


def to_rows(tensor):
    return tensor.transpose(1, 2, 0, 3).reshape(NQB * BLOCK, H * DH)


def reference(queries, keys, values, attended, cotangent, log_totals, block_picks, normed):
    causal = jnp.tril(jnp.ones((BLOCK, BLOCK), bool))
    log_heads = log_totals.reshape(H, NQB, BLOCK)

    def per_head(operands):
        q_h, k_h, v_h, o_h, g_h, l_h, picked = operands
        row_dots = jnp.sum(g_h * o_h, axis=-1)
        dq_diag, dk_diag, dv_diag = tile_grads(q_h, k_h, v_h, g_h, l_h, row_dots, causal)
        present = picked >= 0
        clamped = jnp.maximum(picked, 0)
        k_sel = k_h[clamped]
        v_sel = v_h[clamped]
        tile_shape = k_sel.shape
        q_rep = jnp.broadcast_to(q_h[:, None], tile_shape)
        g_rep = jnp.broadcast_to(g_h[:, None], tile_shape)
        l_rep = jnp.broadcast_to(l_h[:, None], tile_shape[:3])
        d_rep = jnp.broadcast_to(row_dots[:, None], tile_shape[:3])
        allowed = jnp.broadcast_to(present[:, :, None, None], tile_shape[:3] + (BLOCK,))
        dq_sel, dk_sel, dv_sel = tile_grads(q_rep, k_sel, v_sel, g_rep, l_rep, d_rep, allowed)
        segments = jnp.where(present, picked, NQB).reshape(-1).astype(jnp.int32)
        dk_sum = jax.ops.segment_sum(dk_sel.reshape(-1, BLOCK, DH), segments, num_segments=NQB + 1)[:NQB]
        dv_sum = jax.ops.segment_sum(dv_sel.reshape(-1, BLOCK, DH), segments, num_segments=NQB + 1)[:NQB]
        return dq_diag + jnp.sum(dq_sel, axis=1), dk_diag + dk_sum, dv_diag + dv_sum

    grad_q, grad_k, grad_v = lax.map(per_head, (by_head(queries), by_head(keys), by_head(values),
                                                by_head(attended), by_head(cotangent), log_heads, block_picks))
    grad_queries = to_rows(grad_q).astype(jnp.bfloat16)
    grad_weight = jnp.dot(normed.T, grad_queries, preferred_element_type=jnp.float32)
    return grad_queries, to_rows(grad_k).astype(jnp.bfloat16), to_rows(grad_v).astype(jnp.bfloat16), grad_weight
```

```python
import functools

import jax
import jax.numpy as jnp
from jax import lax
from jax.experimental import pallas as pl
from jax.experimental.pallas import tpu as pltpu
from jax.sharding import PartitionSpec as P

BLOCK = 64


def tile_terms(q_tile, k_tile, v_tile, g_tile, log_total, row_dots, allowed):
    scale = q_tile.shape[-1] ** (-0.5)
    scores = (
        jnp.einsum("...qd,...kd->...qk", q_tile, k_tile, preferred_element_type=jnp.float32) * scale
    )
    probs = jnp.where(allowed, jnp.exp(scores - log_total[..., None]), 0.0)
    probs_low = probs.astype(jnp.bfloat16)
    grad_v = jnp.einsum("...qk,...qd->...kd", probs_low, g_tile, preferred_element_type=jnp.float32)
    grad_p = jnp.einsum("...qd,...kd->...qk", g_tile, v_tile, preferred_element_type=jnp.float32)
    grad_s = (probs * (grad_p - row_dots[..., None])).astype(jnp.bfloat16)
    grad_q = (
        jnp.einsum("...qk,...kd->...qd", grad_s, k_tile, preferred_element_type=jnp.float32) * scale
    )
    grad_k = (
        jnp.einsum("...qk,...qd->...kd", grad_s, q_tile, preferred_element_type=jnp.float32) * scale
    )
    return (grad_q, grad_k, grad_v)


def add_by_block(tiles, segments, block_total):
    onehot = (segments[..., None] == jnp.arange(block_total)).astype(jnp.float32)
    return jnp.einsum("hnb,hnkd->hbkd", onehot, tiles, precision=lax.Precision.HIGHEST)


def local(queries, keys, values, attended, cotangent, log_totals, block_picks, normed):
    tok_rows, row_width = queries.shape
    head_count = log_totals.shape[0]
    head_size = row_width // head_count
    local_blocks = tok_rows // BLOCK
    kv_count = lax.axis_size("kv")
    all_blocks = local_blocks * kv_count

    def by_head(matrix, blocks):
        return matrix.reshape(blocks, BLOCK, head_count, head_size).transpose(2, 0, 1, 3)

    def to_rows(tensor):
        return tensor.transpose(1, 2, 0, 3).reshape(tensor.shape[1] * BLOCK, row_width)

    q_heads = by_head(queries, local_blocks)
    k_heads = by_head(keys, local_blocks)
    v_heads = by_head(values, local_blocks)
    g_heads = by_head(cotangent, local_blocks)
    o_heads = by_head(attended, local_blocks)
    log_heads = log_totals.reshape(head_count, local_blocks, BLOCK)
    row_dots = jnp.einsum("hbqd,hbqd->hbq", g_heads, o_heads, preferred_element_type=jnp.float32)
    causal = jnp.tril(jnp.ones((BLOCK, BLOCK), bool))
    dq_diag, dk_diag, dv_diag = tile_terms(
        q_heads, k_heads, v_heads, g_heads, log_heads, row_dots, causal
    )
    q_all, g_all = (
        lax.all_gather(queries, "kv", axis=0, tiled=True),
        lax.all_gather(cotangent, "kv", axis=0, tiled=True),
    )
    log_all, dots_all = (
        lax.all_gather(log_totals, "kv", axis=1, tiled=True),
        lax.all_gather(row_dots.reshape(head_count, tok_rows), "kv", axis=1, tiled=True),
    )
    picks_all = lax.all_gather(block_picks, "kv", axis=1, tiled=True)
    most = max(2, all_blocks // 4)
    own_ids = lax.axis_index("kv") * local_blocks + jnp.arange(local_blocks)
    matched = jnp.any(picks_all[:, :, :, None] == own_ids, axis=2)
    position = jnp.cumsum(matched.astype(jnp.int32), axis=1) - 1
    slot_hit = matched[..., None] & (position[..., None] == jnp.arange(most))
    listed = jnp.sum(jnp.where(slot_hit, jnp.arange(all_blocks)[None, :, None, None], 0), axis=1)
    filled = jnp.any(slot_hit, axis=1)
    q_blocks = by_head(q_all, all_blocks)
    g_blocks = by_head(g_all, all_blocks)
    log_blocks = log_all.reshape(head_count, all_blocks, BLOCK)
    dots_blocks = dots_all.reshape(head_count, all_blocks, BLOCK)
    q_sel = jax.vmap(lambda t, i: t[i])(q_blocks, listed)
    g_sel = jax.vmap(lambda t, i: t[i])(g_blocks, listed)
    l_sel = jax.vmap(lambda t, i: t[i])(log_blocks, listed)
    d_sel = jax.vmap(lambda t, i: t[i])(dots_blocks, listed)
    tile_shape = q_sel.shape
    k_rep = jnp.broadcast_to(k_heads[:, :, None], tile_shape)
    v_rep = jnp.broadcast_to(v_heads[:, :, None], tile_shape)
    allowed = jnp.broadcast_to(filled[..., None, None], tile_shape[:4] + (BLOCK,))
    dq_sel, dk_sel, dv_sel = tile_terms(q_sel, k_rep, v_rep, g_sel, l_sel, d_sel, allowed)
    grad_k = to_rows(dk_diag + jnp.sum(dk_sel, axis=2))
    grad_v = to_rows(dv_diag + jnp.sum(dv_sel, axis=2))
    segments = jnp.where(filled, listed, all_blocks).reshape(head_count, local_blocks * most)
    dq_blocks = add_by_block(
        dq_sel.reshape(head_count, local_blocks * most, BLOCK, head_size), segments, all_blocks
    )
    dq_full = to_rows(dq_blocks)
    remote_q = lax.psum_scatter(dq_full, "kv", scatter_dimension=0, tiled=True)
    grad_queries = (remote_q + to_rows(dq_diag)).astype(jnp.bfloat16)
    full_hidden = lax.all_gather(normed, "tp", axis=1, tiled=True)
    grad_weight = lax.psum_scatter(
        lax.dot_general(
            full_hidden, grad_queries, (((0,), (0,)), ((), ())), preferred_element_type=jnp.float32
        ),
        "kv",
        scatter_dimension=0,
        tiled=True,
    )
    return (grad_queries, grad_k.astype(jnp.bfloat16), grad_v.astype(jnp.bfloat16), grad_weight)


def head_grads(q, k, v, g, log_total, row_dots, picks):
    rows = q.shape[0]
    blocks = rows // BLOCK
    scale = q.shape[-1] ** (-0.5)
    contract_last = (((1,), (1,)), ((), ()))
    contract_first = (((0,), (0,)), ((), ()))
    chosen = jnp.any(picks[:, :, None] == jnp.arange(blocks), axis=1)
    position = jnp.arange(rows)
    chosen = jnp.repeat(jnp.repeat(chosen, BLOCK, axis=0), BLOCK, axis=1)
    own = (position[:, None] // BLOCK == position[None, :] // BLOCK) & (
        position[:, None] >= position[None, :]
    )
    scores = lax.dot_general(q, k, contract_last, preferred_element_type=jnp.float32) * scale
    probs = jnp.where(chosen | own, jnp.exp(scores - log_total[:, None]), 0.0)
    grad_p = lax.dot_general(g, v, contract_last, preferred_element_type=jnp.float32)
    grad_s = (probs * (grad_p - row_dots[:, None])).astype(jnp.bfloat16)
    grad_v = lax.dot_general(
        probs.astype(jnp.bfloat16), g, contract_first, preferred_element_type=jnp.float32
    )
    grad_k = lax.dot_general(grad_s, q, contract_first, preferred_element_type=jnp.float32) * scale
    grad_q = jnp.dot(grad_s, k, preferred_element_type=jnp.float32) * scale
    return grad_q.astype(jnp.bfloat16), grad_k.astype(jnp.bfloat16), grad_v.astype(jnp.bfloat16)


def by_heads(queries, keys, values, attended, cotangent, log_totals, block_picks, normed):
    tok_rows, row_width = queries.shape
    head_count = log_totals.shape[0]
    head_size = row_width // head_count
    kv_count = lax.axis_size("kv")
    heads = head_count // kv_count
    product = cotangent.astype(jnp.float32) * attended.astype(jnp.float32)
    row_dots = jnp.sum(product.reshape(tok_rows, head_count, head_size), axis=2).T
    packed = lax.all_to_all(
        jnp.stack([queries, keys, values, cotangent]), "kv", split_axis=2, concat_axis=1, tiled=True
    )
    sides = lax.all_to_all(
        jnp.stack([log_totals, row_dots]), "kv", split_axis=1, concat_axis=2, tiled=True
    )
    picks = lax.all_to_all(block_picks, "kv", split_axis=0, concat_axis=1, tiled=True)
    features = lax.all_gather(normed, "tp", axis=1, tiled=True)
    features = lax.all_to_all(features, "kv", split_axis=1, concat_axis=0, tiled=True)
    grads = []
    for h in range(heads):
        q, k, v, g = (packed[i, :, h * head_size : (h + 1) * head_size] for i in range(4))
        grads.append(head_grads(q, k, v, g, sides[0, h], sides[1, h], picks[h]))
    dq, dk, dv = (jnp.concatenate(parts, axis=1) for parts in zip(*grads))
    dq_all = lax.all_gather(dq, "kv", axis=1, tiled=True)
    dkv = lax.all_to_all(jnp.stack([dk, dv]), "kv", split_axis=1, concat_axis=2, tiled=True)
    grad_queries = lax.dynamic_slice_in_dim(
        dq_all, lax.axis_index("kv") * tok_rows, tok_rows, axis=0
    )
    grad_weight = lax.dot_general(
        features, dq_all, (((0,), (0,)), ((), ())), preferred_element_type=jnp.float32
    )
    return (grad_queries, dkv[0], dkv[1], grad_weight)


NEVER = -1e30
LAST = (((1,), (1,)), ((), ()))
FIRST = (((0,), (0,)), ((), ()))


def mm(a, b, dims=(((1,), (0,)), ((), ()))):
    return lax.dot_general(a, b, dims, preferred_element_type=jnp.float32)


def remote(src, dst, send, recv, kv, tp):
    return pltpu.make_async_remote_copy(
        src_ref=src,
        dst_ref=dst,
        send_sem=send,
        recv_sem=recv,
        device_id=(kv, tp),
        device_id_type=pl.DeviceIdType.MESH,
    )


def one_head_kernel(
    kvs, tps, q_hbm, k_hbm, v_hbm, g_hbm, o_hbm, log_hbm, picks_hbm, n_hbm,
    gq_ref, gk_ref, gv_ref, gw_ref,
    q_ref, k_ref, v_ref, g_ref, o_ref, log_ref, picks_ref, n_ref, load,
    sent, sent_side, got, got_side, turned, feats, total, dq_all, dkv, dkv_got,
    in_send, in_recv, side_send, side_recv, n1_send, n1_recv, n2_send, n2_recv,
    up_send, down_send, mate_send, line_recv, mate_recv, dkv_send, dkv_recv,
):
    me, tp = lax.axis_index("kv"), lax.axis_index("tp")
    rows, width = q_ref.shape
    hs = width // kvs
    per = rows // BLOCK
    scale = hs ** (-0.5)
    ratio = kvs // tps
    part = feats.shape[1]

    loads = []
    pairs = ((q_hbm, q_ref), (k_hbm, k_ref), (v_hbm, v_ref), (g_hbm, g_ref), (o_hbm, o_ref))
    pairs += ((log_hbm, log_ref), (picks_hbm, picks_ref), (n_hbm, n_ref))
    for at, (source, place) in enumerate(pairs):
        loads.append(pltpu.make_async_copy(source, place, load.at[at]))
        loads[-1].start()

    barrier = pltpu.get_barrier_semaphore()
    count = kvs * tps

    def greet(step, carry):
        other = lax.rem(me * tps + tp + step, count)
        pl.semaphore_signal(
            barrier,
            inc=1,
            device_id=(other // tps, lax.rem(other, tps)),
            device_id_type=pl.DeviceIdType.MESH,
        )
        return carry

    lax.fori_loop(1, count, greet, 0)
    for copy in loads[:-1]:
        copy.wait()

    for h in range(kvs):
        c = slice(h * hs, (h + 1) * hs)
        sent[h, :, : 2 * hs] = jnp.concatenate([q_ref[:, c], k_ref[:, c]], axis=1)
        sent[h, :, 2 * hs :] = jnp.concatenate([v_ref[:, c], g_ref[:, c]], axis=1)
    product = g_ref[...].astype(jnp.float32) * o_ref[...].astype(jnp.float32)
    high = product.astype(jnp.bfloat16)
    low = (product - high.astype(jnp.float32)).astype(jnp.bfloat16)
    head_of = lax.broadcasted_iota(jnp.int32, (16, width), 1) // hs
    pick = (head_of == lax.broadcasted_iota(jnp.int32, (16, width), 0)).astype(jnp.bfloat16)
    dots = mm(pick, high, LAST) + mm(pick, low, LAST)
    line = lax.broadcasted_iota(jnp.int32, (8, rows), 0)
    block_at = lax.broadcasted_iota(jnp.int32, (8, rows), 1) // BLOCK
    for h in range(kvs):
        lines = jnp.where(line == 1, dots[h : h + 1], -log_ref[h : h + 1])
        for b in range(per):
            named = picks_ref[h, b : b + 1]
            bit = jnp.where(named >= 0, jnp.left_shift(1, jnp.maximum(named, 0)), 0)
            bits = jnp.sum(bit.astype(jnp.float32), axis=1, keepdims=True)
            here_in = jnp.logical_and(line == 2, block_at == b)
            lines = jnp.where(here_in, bits, lines)
        sent_side[h] = lines
    got[me] = sent[me]
    got_side[me] = sent_side[me]

    pl.semaphore_wait(barrier, count - 1)

    waits = []
    for d in range(1, kvs):
        to = lax.rem(me + d, kvs)
        side = remote(
            sent_side.at[to], got_side.at[me], side_send.at[d], side_recv.at[d], to, tp
        )
        main = remote(sent.at[to], got.at[me], in_send.at[d], in_recv.at[d], to, tp)
        side.start()
        main.start()
        waits += [side, main]

    loads[-1].wait()
    for b in range(n_ref.shape[1] // 128):
        c = slice(b * 128, (b + 1) * 128)
        turned[c, :] = n_ref[:, c].astype(jnp.float32).T.astype(jnp.bfloat16)
    here = pl.ds(pl.multiple_of(me * rows, rows), rows)

    def n1_copy(h, j):
        place = (h * tps + j) * part
        return remote(
            turned.at[pl.ds(place, part)],
            feats.at[j, :, here],
            n1_send.at[h * tps + j],
            n1_recv.at[me],
            ratio * tp + h,
            j,
        )

    for h in range(ratio):
        for j in range(tps):
            mine = jnp.logical_and(me == ratio * tp + h, tp == j)

            @pl.when(jnp.logical_not(mine))
            def _():
                n1_copy(h, j).start()

            @pl.when(mine)
            def _():
                place = (h * tps + j) * part
                feats[j, :, here] = turned[place : place + part, :]

    for d in range(1, kvs):
        src = lax.rem(me + kvs - d, kvs)
        remote(
            sent_side.at[src], got_side.at[src], side_send.at[d], side_recv.at[d], src, tp
        ).wait_recv()
        remote(sent.at[src], got.at[src], in_send.at[d], in_recv.at[d], src, tp).wait_recv()

    s_at = lax.broadcasted_iota(jnp.int32, (rows, rows), 0)
    t_at = lax.broadcasted_iota(jnp.int32, (rows, rows), 1)
    own = jnp.logical_and(s_at // BLOCK == t_at // BLOCK, s_at <= t_at)
    lines = [
        jnp.concatenate([got_side[m, r : r + 1] for m in range(kvs)], axis=1) for r in range(3)
    ]
    for i in range(kvs):
        late = (kvs - i) * rows
        q = got[i:, :, :hs].reshape(late, hs)
        g = got[i:, :, 3 * hs :].reshape(late, hs)
        k = got[i, :, hs : 2 * hs]
        v = got[i, :, 2 * hs : 3 * hs]

        minus, dots, bits = (r[:, i * rows :] for r in lines)
        bits = bits.astype(jnp.int32)
        parts = []
        for b in range(per):
            named = jnp.bitwise_and(lax.shift_right_logical(bits, i * per + b), 1) == 1
            parts.append(jnp.broadcast_to(jnp.where(named, minus, NEVER), (BLOCK, late)))
        bias = jnp.concatenate(parts, axis=0)
        first = jnp.where(own, minus[:, :rows], bias[:, :rows])
        bias = first if i == kvs - 1 else jnp.concatenate([first, bias[:, rows:]], axis=1)
        probs = jnp.exp(mm(k, q, LAST) * scale + bias)
        grad_s = (probs * (mm(v, g, LAST) - dots)).astype(jnp.bfloat16)
        grad_v = mm(probs.astype(jnp.bfloat16), g)
        grad_k = mm(grad_s, q) * scale
        dkv[i] = jnp.concatenate([grad_k, grad_v], axis=1).astype(jnp.bfloat16)
        grad_q = mm(k, grad_s, FIRST)
        if i == 0:
            total[...] = grad_q
        else:
            total[:, i * rows :] += grad_q
    dq_all[me] = (total[...] * scale).astype(jnp.bfloat16)
    dkv_got[me] = dkv[me]

    deep = kvs // 2
    spot, side_of = me // 2, lax.rem(me, 2)
    mate = me + 1 - 2 * side_of
    half = hs // 2
    not_top, not_bottom = spot < deep - 1, spot > 0

    def unit_copy(unit, piece, send, recv, column, to):
        rows_of = dq_all.at[unit * 2 + column, piece * half : (piece + 1) * half]
        at = unit * 2 + piece
        return remote(rows_of, rows_of, send.at[at], recv.at[at], to, tp)

    def upward(unit, piece):
        return unit_copy(unit, piece, up_send, line_recv, side_of, me + 2)

    def downward(unit, piece):
        return unit_copy(unit, piece, down_send, line_recv, side_of, me - 2)

    def across(unit, piece):
        return unit_copy(unit, piece, mate_send, mate_recv, side_of, mate)

    for piece in range(2):

        @pl.when(not_top)
        def _():
            upward(spot, piece).start()

        @pl.when(not_bottom)
        def _():
            downward(spot, piece).start()

    for piece in range(2):
        across(spot, piece).start()
    for d in range(1, kvs):
        to = lax.rem(me + d, kvs)
        copy = remote(dkv.at[to], dkv_got.at[me], dkv_send.at[d], dkv_recv.at[d], to, tp)
        copy.start()
        waits.append(copy)

    for k in range(kvs):

        @pl.when(jnp.logical_not(jnp.logical_and(me == k, tp == me // ratio)))
        def _():
            remote(
                turned.at[pl.ds(0, part)],
                feats.at[tp, :, pl.ds(k * rows, rows)],
                n1_send.at[0],
                n1_recv.at[k],
                me,
                tp,
            ).wait_recv()

    for d in range(1, tps):
        to = lax.rem(tp + d, tps)
        copy = remote(feats.at[tp], feats.at[tp], n2_send.at[d], n2_recv.at[d], me, to)
        copy.start()
        waits.append(copy)

    for z in range(1, deep):
        for piece in range(2):

            @pl.when(spot >= z)
            def _():
                unit_copy(spot - z, piece, up_send, line_recv, side_of, me).wait_recv()

                @pl.when(not_top)
                def _():
                    upward(spot - z, piece).start()

                across(spot - z, piece).start()

            @pl.when(spot + z < deep)
            def _():
                unit_copy(spot + z, piece, down_send, line_recv, side_of, me).wait_recv()

                @pl.when(not_bottom)
                def _():
                    downward(spot + z, piece).start()

                across(spot + z, piece).start()

    for d in range(1, kvs):
        src = lax.rem(me + kvs - d, kvs)
        remote(
            dkv.at[src], dkv_got.at[src], dkv_send.at[d], dkv_recv.at[d], src, tp
        ).wait_recv()
    for p in range(kvs // 2):
        c = slice(p * 2 * hs, (p + 1) * 2 * hs)
        left, right = dkv_got[2 * p], dkv_got[2 * p + 1]
        gk_ref[:, c] = jnp.concatenate([left[:, :hs], right[:, :hs]], axis=1)
        gv_ref[:, c] = jnp.concatenate([left[:, hs:], right[:, hs:]], axis=1)

    for d in range(1, tps):
        src = lax.rem(tp + tps - d, tps)
        remote(
            feats.at[src], feats.at[src], n2_send.at[d], n2_recv.at[d], me, src
        ).wait_recv()
    step = jnp.where(spot < deep // 2, 1, deep - 1)
    for z in range(deep):
        unit = lax.rem(spot + z * step, deep)
        for piece in range(2):
            unit_copy(unit, piece, mate_send, mate_recv, 1 - side_of, me).wait_recv()
        c = pl.ds(pl.multiple_of(unit * 2 * hs, 2 * hs), 2 * hs)
        pair = dq_all[pl.ds(unit * 2, 2), :, here].reshape(2 * hs, rows)
        gq_ref[:, c] = pair.astype(jnp.float32).T.astype(jnp.bfloat16)
        cols = dq_all[pl.ds(unit * 2, 2)].reshape(2 * hs, kvs * rows)
        for j in range(tps):
            gw_ref[j * part : (j + 1) * part, c] = mm(feats[j], cols, LAST)

    for unit in range(deep):
        for piece in range(2):
            across(unit, piece).wait_send()

            @pl.when(jnp.logical_and(not_top, unit <= spot))
            def _():
                upward(unit, piece).wait_send()

            @pl.when(jnp.logical_and(not_bottom, unit >= spot))
            def _():
                downward(unit, piece).wait_send()

    for copy in waits:
        copy.wait_send()
    for h in range(ratio):
        for j in range(tps):
            mine = jnp.logical_and(me == ratio * tp + h, tp == j)

            @pl.when(jnp.logical_not(mine))
            def _():
                n1_copy(h, j).wait_send()


def finish_kernel(count, *refs):
    sources, places, done = refs[:count], refs[count : 2 * count], refs[2 * count]
    copies = [
        pltpu.make_async_copy(source, place, done.at[at])
        for at, (source, place) in enumerate(zip(sources, places))
    ]
    for copy in copies[::-1]:
        copy.start()
    for copy in copies:
        copy.wait()


def finish(arrays):
    count = len(arrays)
    return pl.pallas_call(
        functools.partial(finish_kernel, count),
        out_shape=tuple(jax.ShapeDtypeStruct(a.shape, a.dtype) for a in arrays),
        in_specs=[pl.BlockSpec(memory_space=pltpu.VMEM)] * count,
        out_specs=(pl.BlockSpec(memory_space=pltpu.HBM),) * count,
        scratch_shapes=[pltpu.SemaphoreType.DMA((count,))],
    )(*[pltpu.with_memory_space_constraint(a, pltpu.VMEM) for a in arrays])


def one_head(queries, keys, values, attended, cotangent, log_totals, block_picks, normed):
    arrays = (queries, keys, values, cotangent, attended, log_totals, block_picks, normed)
    rows, width = queries.shape
    kvs, tps = lax.axis_size("kv"), lax.axis_size("tp")
    hs = width // kvs
    local_width = normed.shape[1]
    part = local_width // kvs
    vmem = pl.BlockSpec(memory_space=pltpu.VMEM)
    dma = pltpu.SemaphoreType.DMA
    low = jnp.bfloat16
    outs = pl.pallas_call(
        functools.partial(one_head_kernel, kvs, tps),
        out_shape=(
            pltpu.VMEM((rows, width), low),
            pltpu.VMEM((rows, width), low),
            pltpu.VMEM((rows, width), low),
            pltpu.VMEM((tps * part, width), jnp.float32),
        ),
        in_specs=[pl.BlockSpec(memory_space=pl.ANY)] * 8,
        out_specs=(vmem,) * 4,
        scratch_shapes=[pltpu.VMEM((rows, width), low)] * 5
        + [
            pltpu.VMEM(log_totals.shape, jnp.float32),
            pltpu.VMEM(block_picks.shape, jnp.int32),
            pltpu.VMEM((rows, local_width), low),
            dma((8,)),
        ]
        + [
            pltpu.VMEM((kvs, rows, 4 * hs), low),
            pltpu.VMEM((kvs, 8, rows), jnp.float32),
            pltpu.VMEM((kvs, rows, 4 * hs), low),
            pltpu.VMEM((kvs, 8, rows), jnp.float32),
            pltpu.VMEM((local_width, rows), low),
            pltpu.VMEM((tps, part, kvs * rows), low),
            pltpu.VMEM((hs, kvs * rows), jnp.float32),
            pltpu.VMEM((kvs, hs, kvs * rows), low),
            pltpu.VMEM((kvs, rows, 2 * hs), low),
            pltpu.VMEM((kvs, rows, 2 * hs), low),
        ]
        + [dma((kvs,))] * 6
        + [dma((tps,))] * 2
        + [dma((kvs,))] * 7,
        compiler_params=pltpu.CompilerParams(
            collective_id=0, has_side_effects=True, vmem_limit_bytes=40 * 2**20
        ),
    )(*[pltpu.with_memory_space_constraint(a, pltpu.HBM) for a in arrays])
    return finish(outs)


def device_part(*arrays):
    heads, kvs, tps = arrays[5].shape[0], lax.axis_size("kv"), lax.axis_size("tp")
    rows, width = arrays[0].shape
    if heads == kvs and kvs % (2 * tps) == 0 and rows == 2 * width // heads == 128 and kvs <= 8:
        return one_head(*arrays)
    if heads % kvs == 0:
        return by_heads(*arrays)
    return local(*arrays)


def solution(mesh):
    in_specs = (
        P("kv", "tp"),
        P("kv", "tp"),
        P("kv", "tp"),
        P("kv", "tp"),
        P("kv", "tp"),
        P("tp", "kv"),
        P("tp", "kv", None),
        P("kv", "tp"),
    )
    out_specs = (P("kv", "tp"), P("kv", "tp"), P("kv", "tp"), P("kv", "tp"))
    return jax.shard_map(device_part, mesh=mesh, in_specs=in_specs, out_specs=out_specs, check_vma=False)
```

```python
import functools

import jax
import jax.numpy as jnp
from jax import lax
from jax.experimental import pallas as pl
from jax.experimental.pallas import tpu as pltpu
from jax.sharding import PartitionSpec as P

BLOCK = 64


def tile_terms(q_tile, k_tile, v_tile, g_tile, log_total, row_dots, allowed):
    scale = q_tile.shape[-1] ** (-0.5)
    scores = (
        jnp.einsum("...qd,...kd->...qk", q_tile, k_tile, preferred_element_type=jnp.float32) * scale
    )
    probs = jnp.where(allowed, jnp.exp(scores - log_total[..., None]), 0.0)
    probs_low = probs.astype(jnp.bfloat16)
    grad_v = jnp.einsum("...qk,...qd->...kd", probs_low, g_tile, preferred_element_type=jnp.float32)
    grad_p = jnp.einsum("...qd,...kd->...qk", g_tile, v_tile, preferred_element_type=jnp.float32)
    grad_s = (probs * (grad_p - row_dots[..., None])).astype(jnp.bfloat16)
    grad_q = (
        jnp.einsum("...qk,...kd->...qd", grad_s, k_tile, preferred_element_type=jnp.float32) * scale
    )
    grad_k = (
        jnp.einsum("...qk,...qd->...kd", grad_s, q_tile, preferred_element_type=jnp.float32) * scale
    )
    return (grad_q, grad_k, grad_v)


def add_by_block(tiles, segments, block_total):
    onehot = (segments[..., None] == jnp.arange(block_total)).astype(jnp.float32)
    return jnp.einsum("hnb,hnkd->hbkd", onehot, tiles, precision=lax.Precision.HIGHEST)


def local(queries, keys, values, attended, cotangent, log_totals, block_picks, normed):
    tok_rows, row_width = queries.shape
    head_count = log_totals.shape[0]
    head_size = row_width // head_count
    local_blocks = tok_rows // BLOCK
    kv_count = lax.axis_size("kv")
    all_blocks = local_blocks * kv_count

    def by_head(matrix, blocks):
        return matrix.reshape(blocks, BLOCK, head_count, head_size).transpose(2, 0, 1, 3)

    def to_rows(tensor):
        return tensor.transpose(1, 2, 0, 3).reshape(tensor.shape[1] * BLOCK, row_width)

    q_heads = by_head(queries, local_blocks)
    k_heads = by_head(keys, local_blocks)
    v_heads = by_head(values, local_blocks)
    g_heads = by_head(cotangent, local_blocks)
    o_heads = by_head(attended, local_blocks)
    log_heads = log_totals.reshape(head_count, local_blocks, BLOCK)
    row_dots = jnp.einsum("hbqd,hbqd->hbq", g_heads, o_heads, preferred_element_type=jnp.float32)
    causal = jnp.tril(jnp.ones((BLOCK, BLOCK), bool))
    dq_diag, dk_diag, dv_diag = tile_terms(
        q_heads, k_heads, v_heads, g_heads, log_heads, row_dots, causal
    )
    q_all, g_all = (
        lax.all_gather(queries, "kv", axis=0, tiled=True),
        lax.all_gather(cotangent, "kv", axis=0, tiled=True),
    )
    log_all, dots_all = (
        lax.all_gather(log_totals, "kv", axis=1, tiled=True),
        lax.all_gather(row_dots.reshape(head_count, tok_rows), "kv", axis=1, tiled=True),
    )
    picks_all = lax.all_gather(block_picks, "kv", axis=1, tiled=True)
    most = max(2, all_blocks // 4)
    own_ids = lax.axis_index("kv") * local_blocks + jnp.arange(local_blocks)
    matched = jnp.any(picks_all[:, :, :, None] == own_ids, axis=2)
    position = jnp.cumsum(matched.astype(jnp.int32), axis=1) - 1
    slot_hit = matched[..., None] & (position[..., None] == jnp.arange(most))
    listed = jnp.sum(jnp.where(slot_hit, jnp.arange(all_blocks)[None, :, None, None], 0), axis=1)
    filled = jnp.any(slot_hit, axis=1)
    q_blocks = by_head(q_all, all_blocks)
    g_blocks = by_head(g_all, all_blocks)
    log_blocks = log_all.reshape(head_count, all_blocks, BLOCK)
    dots_blocks = dots_all.reshape(head_count, all_blocks, BLOCK)
    q_sel = jax.vmap(lambda t, i: t[i])(q_blocks, listed)
    g_sel = jax.vmap(lambda t, i: t[i])(g_blocks, listed)
    l_sel = jax.vmap(lambda t, i: t[i])(log_blocks, listed)
    d_sel = jax.vmap(lambda t, i: t[i])(dots_blocks, listed)
    tile_shape = q_sel.shape
    k_rep = jnp.broadcast_to(k_heads[:, :, None], tile_shape)
    v_rep = jnp.broadcast_to(v_heads[:, :, None], tile_shape)
    allowed = jnp.broadcast_to(filled[..., None, None], tile_shape[:4] + (BLOCK,))
    dq_sel, dk_sel, dv_sel = tile_terms(q_sel, k_rep, v_rep, g_sel, l_sel, d_sel, allowed)
    grad_k = to_rows(dk_diag + jnp.sum(dk_sel, axis=2))
    grad_v = to_rows(dv_diag + jnp.sum(dv_sel, axis=2))
    segments = jnp.where(filled, listed, all_blocks).reshape(head_count, local_blocks * most)
    dq_blocks = add_by_block(
        dq_sel.reshape(head_count, local_blocks * most, BLOCK, head_size), segments, all_blocks
    )
    dq_full = to_rows(dq_blocks)
    remote_q = lax.psum_scatter(dq_full, "kv", scatter_dimension=0, tiled=True)
    grad_queries = (remote_q + to_rows(dq_diag)).astype(jnp.bfloat16)
    full_hidden = lax.all_gather(normed, "tp", axis=1, tiled=True)
    grad_weight = lax.psum_scatter(
        lax.dot_general(
            full_hidden, grad_queries, (((0,), (0,)), ((), ())), preferred_element_type=jnp.float32
        ),
        "kv",
        scatter_dimension=0,
        tiled=True,
    )
    return (grad_queries, grad_k.astype(jnp.bfloat16), grad_v.astype(jnp.bfloat16), grad_weight)


def head_grads(q, k, v, g, log_total, row_dots, picks):
    rows = q.shape[0]
    blocks = rows // BLOCK
    scale = q.shape[-1] ** (-0.5)
    contract_last = (((1,), (1,)), ((), ()))
    contract_first = (((0,), (0,)), ((), ()))
    chosen = jnp.any(picks[:, :, None] == jnp.arange(blocks), axis=1)
    position = jnp.arange(rows)
    chosen = jnp.repeat(jnp.repeat(chosen, BLOCK, axis=0), BLOCK, axis=1)
    own = (position[:, None] // BLOCK == position[None, :] // BLOCK) & (
        position[:, None] >= position[None, :]
    )
    scores = lax.dot_general(q, k, contract_last, preferred_element_type=jnp.float32) * scale
    probs = jnp.where(chosen | own, jnp.exp(scores - log_total[:, None]), 0.0)
    grad_p = lax.dot_general(g, v, contract_last, preferred_element_type=jnp.float32)
    grad_s = (probs * (grad_p - row_dots[:, None])).astype(jnp.bfloat16)
    grad_v = lax.dot_general(
        probs.astype(jnp.bfloat16), g, contract_first, preferred_element_type=jnp.float32
    )
    grad_k = lax.dot_general(grad_s, q, contract_first, preferred_element_type=jnp.float32) * scale
    grad_q = jnp.dot(grad_s, k, preferred_element_type=jnp.float32) * scale
    return grad_q.astype(jnp.bfloat16), grad_k.astype(jnp.bfloat16), grad_v.astype(jnp.bfloat16)


def by_heads(queries, keys, values, attended, cotangent, log_totals, block_picks, normed):
    tok_rows, row_width = queries.shape
    head_count = log_totals.shape[0]
    head_size = row_width // head_count
    kv_count = lax.axis_size("kv")
    heads = head_count // kv_count
    product = cotangent.astype(jnp.float32) * attended.astype(jnp.float32)
    row_dots = jnp.sum(product.reshape(tok_rows, head_count, head_size), axis=2).T
    packed = lax.all_to_all(
        jnp.stack([queries, keys, values, cotangent]), "kv", split_axis=2, concat_axis=1, tiled=True
    )
    sides = lax.all_to_all(
        jnp.stack([log_totals, row_dots]), "kv", split_axis=1, concat_axis=2, tiled=True
    )
    picks = lax.all_to_all(block_picks, "kv", split_axis=0, concat_axis=1, tiled=True)
    features = lax.all_gather(normed, "tp", axis=1, tiled=True)
    features = lax.all_to_all(features, "kv", split_axis=1, concat_axis=0, tiled=True)
    grads = []
    for h in range(heads):
        q, k, v, g = (packed[i, :, h * head_size : (h + 1) * head_size] for i in range(4))
        grads.append(head_grads(q, k, v, g, sides[0, h], sides[1, h], picks[h]))
    dq, dk, dv = (jnp.concatenate(parts, axis=1) for parts in zip(*grads))
    dq_all = lax.all_gather(dq, "kv", axis=1, tiled=True)
    dkv = lax.all_to_all(jnp.stack([dk, dv]), "kv", split_axis=1, concat_axis=2, tiled=True)
    grad_queries = lax.dynamic_slice_in_dim(
        dq_all, lax.axis_index("kv") * tok_rows, tok_rows, axis=0
    )
    grad_weight = lax.dot_general(
        features, dq_all, (((0,), (0,)), ((), ())), preferred_element_type=jnp.float32
    )
    return (grad_queries, dkv[0], dkv[1], grad_weight)


NEVER = -1e30
LAST = (((1,), (1,)), ((), ()))
FIRST = (((0,), (0,)), ((), ()))


def mm(a, b, dims=(((1,), (0,)), ((), ()))):
    return lax.dot_general(a, b, dims, preferred_element_type=jnp.float32)


def remote(src, dst, send, recv, kv, tp):
    return pltpu.make_async_remote_copy(
        src_ref=src,
        dst_ref=dst,
        send_sem=send,
        recv_sem=recv,
        device_id=(kv, tp),
        device_id_type=pl.DeviceIdType.MESH,
    )


def one_head_kernel(
    kvs, tps, q_hbm, k_hbm, v_hbm, g_hbm, o_hbm, log_hbm, picks_hbm, n_hbm,
    gq_ref, gk_ref, gv_ref, gw_ref,
    q_ref, k_ref, v_ref, g_ref, o_ref, log_ref, picks_ref, n_ref, load,
    sent, sent_side, got, got_side, turned, plane, feats, total, dq_all, dkv, dkv_got,
    in_send, in_recv, side_send, side_recv, n1_send, n1_recv, n2_send, n2_recv,
    y_send, y_recv, core_send, core_recv,
    up_send, down_send, mate_send, line_recv, mate_recv, dkv_send, dkv_recv,
):
    me, tp = lax.axis_index("kv"), lax.axis_index("tp")
    rows, width = q_ref.shape
    hs = width // kvs
    per = rows // BLOCK
    scale = hs ** (-0.5)
    part = feats.shape[1]

    loads = []
    pairs = ((q_hbm, q_ref), (k_hbm, k_ref), (v_hbm, v_ref), (g_hbm, g_ref), (o_hbm, o_ref))
    pairs += ((log_hbm, log_ref), (picks_hbm, picks_ref), (n_hbm, n_ref))
    for at, (source, place) in enumerate(pairs):
        loads.append(pltpu.make_async_copy(source, place, load.at[at]))
        loads[-1].start()

    barrier = pltpu.get_barrier_semaphore()
    deep = kvs // 2
    spot, side_of = me // 2, lax.rem(me, 2)
    mate = me + 1 - 2 * side_of
    partners = [(lax.rem(me + d, kvs), tp) for d in range(1, kvs)]
    partners += [(to, lax.rem(tp + d, tps)) for d in range(1, tps) for to in (me, mate)]
    for partner in partners:
        pl.semaphore_signal(
            barrier, inc=1, device_id=partner, device_id_type=pl.DeviceIdType.MESH
        )
    for copy in loads[:-1]:
        copy.wait()

    for h in range(kvs):
        c = slice(h * hs, (h + 1) * hs)
        sent[h, :, : 2 * hs] = jnp.concatenate([q_ref[:, c], k_ref[:, c]], axis=1)
        sent[h, :, 2 * hs :] = jnp.concatenate([v_ref[:, c], g_ref[:, c]], axis=1)
    product = g_ref[...].astype(jnp.float32) * o_ref[...].astype(jnp.float32)
    high = product.astype(jnp.bfloat16)
    low = (product - high.astype(jnp.float32)).astype(jnp.bfloat16)
    head_of = lax.broadcasted_iota(jnp.int32, (16, width), 1) // hs
    pick = (head_of == lax.broadcasted_iota(jnp.int32, (16, width), 0)).astype(jnp.bfloat16)
    dots = mm(pick, high, LAST) + mm(pick, low, LAST)
    line = lax.broadcasted_iota(jnp.int32, (8, rows), 0)
    block_at = lax.broadcasted_iota(jnp.int32, (8, rows), 1) // BLOCK
    for h in range(kvs):
        lines = jnp.where(line == 1, dots[h : h + 1], -log_ref[h : h + 1])
        for b in range(per):
            named = picks_ref[h, b : b + 1]
            bit = jnp.where(named >= 0, jnp.left_shift(1, jnp.maximum(named, 0)), 0)
            bits = jnp.sum(bit.astype(jnp.float32), axis=1, keepdims=True)
            here_in = jnp.logical_and(line == 2, block_at == b)
            lines = jnp.where(here_in, bits, lines)
        sent_side[h] = lines
    got[me] = sent[me]
    got_side[me] = sent_side[me]

    pl.semaphore_wait(barrier, len(partners))

    waits = []
    for d in range(1, kvs):
        to = lax.rem(me + d, kvs)
        side = remote(
            sent_side.at[to], got_side.at[me], side_send.at[d], side_recv.at[d], to, tp
        )
        main = remote(sent.at[to], got.at[me], in_send.at[d], in_recv.at[d], to, tp)
        side.start()
        main.start()
        waits += [side, main]

    loads[-1].wait()
    for b in range(n_ref.shape[1] // 128):
        c = slice(b * 128, (b + 1) * 128)
        turned[c, :] = n_ref[:, c].astype(jnp.float32).T.astype(jnp.bfloat16)
    here = pl.ds(pl.multiple_of(me * rows, rows), rows)

    def side_rows(side):
        return pl.ds(pl.multiple_of(side * rows, rows), rows)

    def plane_rows(level):
        return pl.ds(pl.multiple_of(level * 2 * rows, 2 * rows), 2 * rows)

    def n1_copy(h, j):
        return remote(
            turned.at[pl.ds((h * tps + j) * part, part)],
            plane.at[tp, :, side_rows(side_of)],
            n1_send.at[h * tps + j],
            n1_recv.at[side_of * tps + tp],
            spot * 2 + h,
            j,
        )

    for h in range(2):
        for j in range(tps):
            mine = jnp.logical_and(side_of == h, tp == j)

            @pl.when(jnp.logical_not(mine))
            def _():
                n1_copy(h, j).start()

            @pl.when(mine)
            def _():
                place = (h * tps + j) * part
                plane[j, :, h * rows : (h + 1) * rows] = turned[place : place + part, :]

    for h in range(2):
        for j in range(tps):

            @pl.when(jnp.logical_not(jnp.logical_and(side_of == h, tp == j)))
            def _():
                remote(
                    turned.at[pl.ds(0, part)],
                    plane.at[j, :, side_rows(h)],
                    n1_send.at[0],
                    n1_recv.at[h * tps + j],
                    me,
                    tp,
                ).wait_recv()

    opposite, partner_core = lax.rem(tp + tps // 2, tps), tp + 1 - 2 * lax.rem(tp, 2)

    def level_copy(d, level, at):
        return remote(
            plane.at[level],
            feats.at[tp, :, plane_rows(at)],
            n2_send.at[d],
            n2_recv.at[d],
            level * 2 + side_of,
            tp,
        )

    for d in range(1, deep):
        copy = level_copy(d, lax.rem(spot + d, deep), spot)
        copy.start()
        waits.append(copy)
    feats[tp, :, plane_rows(spot)] = plane[spot]

    def chunk_copy(d, owner, own, send, recv, at, to):
        rows_of = feats.at[owner, :, plane_rows(lax.rem(spot + deep - d, deep))]
        source = plane.at[spot] if own and d == 0 else rows_of
        return remote(source, rows_of, send.at[at], recv.at[at], me, to)

    def over_y(d, owner):
        return chunk_copy(d, owner, True, y_send, y_recv, d, opposite)

    def over_core(d, owner, relayed):
        return chunk_copy(
            d, owner, not relayed, core_send, core_recv, relayed * deep + d, partner_core
        )

    def pass_chunk(d):
        if d:
            level_copy(d, spot, lax.rem(spot + deep - d, deep)).wait_recv()
        for copy in (over_y(d, tp), over_core(d, tp, 0)):
            copy.start()
            waits.append(copy)

    def relay_chunk(d):
        over_y(d, opposite).wait_recv()
        copy = over_core(d, opposite, 1)
        copy.start()
        waits.append(copy)

    pass_chunk(0)

    for d in range(1, kvs):
        src = lax.rem(me + kvs - d, kvs)
        remote(
            sent_side.at[src], got_side.at[src], side_send.at[d], side_recv.at[d], src, tp
        ).wait_recv()
        remote(sent.at[src], got.at[src], in_send.at[d], in_recv.at[d], src, tp).wait_recv()

    s_at = lax.broadcasted_iota(jnp.int32, (rows, rows), 0)
    t_at = lax.broadcasted_iota(jnp.int32, (rows, rows), 1)
    own = jnp.logical_and(s_at // BLOCK == t_at // BLOCK, s_at <= t_at)
    lines = [
        jnp.concatenate([got_side[m, r : r + 1] for m in range(kvs)], axis=1) for r in range(3)
    ]
    for i in range(kvs):
        late = (kvs - i) * rows
        q = got[i:, :, :hs].reshape(late, hs)
        g = got[i:, :, 3 * hs :].reshape(late, hs)
        k = got[i, :, hs : 2 * hs]
        v = got[i, :, 2 * hs : 3 * hs]

        minus, dots, bits = (r[:, i * rows :] for r in lines)
        bits = bits.astype(jnp.int32)
        parts = []
        for b in range(per):
            named = jnp.bitwise_and(lax.shift_right_logical(bits, i * per + b), 1) == 1
            parts.append(jnp.broadcast_to(jnp.where(named, minus, NEVER), (BLOCK, late)))
        bias = jnp.concatenate(parts, axis=0)
        first = jnp.where(own, minus[:, :rows], bias[:, :rows])
        bias = first if i == kvs - 1 else jnp.concatenate([first, bias[:, rows:]], axis=1)
        probs = jnp.exp(mm(k, q, LAST) * scale + bias)
        grad_s = (probs * (mm(v, g, LAST) - dots)).astype(jnp.bfloat16)
        grad_v = mm(probs.astype(jnp.bfloat16), g)
        grad_k = mm(grad_s, q) * scale
        dkv[i] = jnp.concatenate([grad_k, grad_v], axis=1).astype(jnp.bfloat16)
        grad_q = mm(k, grad_s, FIRST)
        if i == 0:
            total[...] = grad_q
        else:
            total[:, i * rows :] += grad_q
    dq_all[me] = (total[...] * scale).astype(jnp.bfloat16)
    dkv_got[me] = dkv[me]

    half = hs // 2
    not_top, not_bottom = spot < deep - 1, spot > 0

    def unit_copy(unit, piece, send, recv, column, to):
        rows_of = dq_all.at[unit * 2 + column, piece * half : (piece + 1) * half]
        at = unit * 2 + piece
        return remote(rows_of, rows_of, send.at[at], recv.at[at], to, tp)

    def upward(unit, piece):
        return unit_copy(unit, piece, up_send, line_recv, side_of, me + 2)

    def downward(unit, piece):
        return unit_copy(unit, piece, down_send, line_recv, side_of, me - 2)

    def across(unit, piece):
        return unit_copy(unit, piece, mate_send, mate_recv, side_of, mate)

    for piece in range(2):

        @pl.when(not_top)
        def _():
            upward(spot, piece).start()

        @pl.when(not_bottom)
        def _():
            downward(spot, piece).start()

    for piece in range(2):
        across(spot, piece).start()
    for d in range(1, kvs):
        to = lax.rem(me + d, kvs)
        copy = remote(dkv.at[to], dkv_got.at[me], dkv_send.at[d], dkv_recv.at[d], to, tp)
        copy.start()
        waits.append(copy)

    for d in range(1, deep):
        pass_chunk(d)

    for z in range(1, deep):
        for piece in range(2):

            @pl.when(spot >= z)
            def _():
                unit_copy(spot - z, piece, up_send, line_recv, side_of, me).wait_recv()

                @pl.when(not_top)
                def _():
                    upward(spot - z, piece).start()

                across(spot - z, piece).start()

            @pl.when(spot + z < deep)
            def _():
                unit_copy(spot + z, piece, down_send, line_recv, side_of, me).wait_recv()

                @pl.when(not_bottom)
                def _():
                    downward(spot + z, piece).start()

                across(spot + z, piece).start()

        relay_chunk(z - 1)
    relay_chunk(deep - 1)

    for d in range(1, kvs):
        src = lax.rem(me + kvs - d, kvs)
        remote(
            dkv.at[src], dkv_got.at[src], dkv_send.at[d], dkv_recv.at[d], src, tp
        ).wait_recv()
    for p in range(kvs // 2):
        c = slice(p * 2 * hs, (p + 1) * 2 * hs)
        left, right = dkv_got[2 * p], dkv_got[2 * p + 1]
        gk_ref[:, c] = jnp.concatenate([left[:, :hs], right[:, :hs]], axis=1)
        gv_ref[:, c] = jnp.concatenate([left[:, hs:], right[:, hs:]], axis=1)

    for d in range(deep):
        over_core(d, partner_core, 0).wait_recv()
        over_core(d, lax.rem(partner_core + tps // 2, tps), 1).wait_recv()
    step = jnp.where(spot < deep // 2, 1, deep - 1)
    for z in range(deep):
        unit = lax.rem(spot + z * step, deep)
        for piece in range(2):
            unit_copy(unit, piece, mate_send, mate_recv, 1 - side_of, me).wait_recv()
        c = pl.ds(pl.multiple_of(unit * 2 * hs, 2 * hs), 2 * hs)
        pair = dq_all[pl.ds(unit * 2, 2), :, here].reshape(2 * hs, rows)
        gq_ref[:, c] = pair.astype(jnp.float32).T.astype(jnp.bfloat16)
        cols = dq_all[pl.ds(unit * 2, 2)].reshape(2 * hs, kvs * rows)
        for j in range(tps):
            gw_ref[j * part : (j + 1) * part, c] = mm(feats[j], cols, LAST)

    for unit in range(deep):
        for piece in range(2):
            across(unit, piece).wait_send()

            @pl.when(jnp.logical_and(not_top, unit <= spot))
            def _():
                upward(unit, piece).wait_send()

            @pl.when(jnp.logical_and(not_bottom, unit >= spot))
            def _():
                downward(unit, piece).wait_send()

    for copy in waits:
        copy.wait_send()
    for h in range(2):
        for j in range(tps):

            @pl.when(jnp.logical_not(jnp.logical_and(side_of == h, tp == j)))
            def _():
                n1_copy(h, j).wait_send()


def finish_kernel(count, *refs):
    sources, places, done = refs[:count], refs[count : 2 * count], refs[2 * count]
    copies = [
        pltpu.make_async_copy(source, place, done.at[at])
        for at, (source, place) in enumerate(zip(sources, places))
    ]
    for copy in copies[::-1]:
        copy.start()
    for copy in copies:
        copy.wait()


def finish(arrays):
    count = len(arrays)
    return pl.pallas_call(
        functools.partial(finish_kernel, count),
        out_shape=tuple(jax.ShapeDtypeStruct(a.shape, a.dtype) for a in arrays),
        in_specs=[pl.BlockSpec(memory_space=pltpu.VMEM)] * count,
        out_specs=(pl.BlockSpec(memory_space=pltpu.HBM),) * count,
        scratch_shapes=[pltpu.SemaphoreType.DMA((count,))],
    )(*[pltpu.with_memory_space_constraint(a, pltpu.VMEM) for a in arrays])


def one_head(queries, keys, values, attended, cotangent, log_totals, block_picks, normed):
    arrays = (queries, keys, values, cotangent, attended, log_totals, block_picks, normed)
    rows, width = queries.shape
    kvs, tps = lax.axis_size("kv"), lax.axis_size("tp")
    hs = width // kvs
    local_width = normed.shape[1]
    part = local_width // kvs
    vmem = pl.BlockSpec(memory_space=pltpu.VMEM)
    dma = pltpu.SemaphoreType.DMA
    low = jnp.bfloat16
    outs = pl.pallas_call(
        functools.partial(one_head_kernel, kvs, tps),
        out_shape=(
            pltpu.VMEM((rows, width), low),
            pltpu.VMEM((rows, width), low),
            pltpu.VMEM((rows, width), low),
            pltpu.VMEM((tps * part, width), jnp.float32),
        ),
        in_specs=[pl.BlockSpec(memory_space=pl.ANY)] * 8,
        out_specs=(vmem,) * 4,
        scratch_shapes=[pltpu.VMEM((rows, width), low)] * 5
        + [
            pltpu.VMEM(log_totals.shape, jnp.float32),
            pltpu.VMEM(block_picks.shape, jnp.int32),
            pltpu.VMEM((rows, local_width), low),
            dma((8,)),
        ]
        + [
            pltpu.VMEM((kvs, rows, 4 * hs), low),
            pltpu.VMEM((kvs, 8, rows), jnp.float32),
            pltpu.VMEM((kvs, rows, 4 * hs), low),
            pltpu.VMEM((kvs, 8, rows), jnp.float32),
            pltpu.VMEM((local_width, rows), low),
            pltpu.VMEM((kvs // 2, part, 2 * rows), low),
            pltpu.VMEM((tps, part, kvs * rows), low),
            pltpu.VMEM((hs, kvs * rows), jnp.float32),
            pltpu.VMEM((kvs, hs, kvs * rows), low),
            pltpu.VMEM((kvs, rows, 2 * hs), low),
            pltpu.VMEM((kvs, rows, 2 * hs), low),
        ]
        + [dma((kvs,))] * 6
        + [dma((kvs // 2,))] * 4
        + [dma((kvs,))] * 9,
        compiler_params=pltpu.CompilerParams(
            collective_id=0, has_side_effects=True, vmem_limit_bytes=40 * 2**20
        ),
    )(*[pltpu.with_memory_space_constraint(a, pltpu.HBM) for a in arrays])
    return finish(outs)


def device_part(*arrays):
    heads, kvs, tps = arrays[5].shape[0], lax.axis_size("kv"), lax.axis_size("tp")
    rows, width = arrays[0].shape
    if heads == kvs and kvs == 2 * tps and tps == 4 and rows == 2 * width // heads == 128 and kvs <= 8:
        return one_head(*arrays)
    if heads % kvs == 0:
        return by_heads(*arrays)
    return local(*arrays)


def solution(mesh):
    in_specs = (
        P("kv", "tp"),
        P("kv", "tp"),
        P("kv", "tp"),
        P("kv", "tp"),
        P("kv", "tp"),
        P("tp", "kv"),
        P("tp", "kv", None),
        P("kv", "tp"),
    )
    out_specs = (P("kv", "tp"), P("kv", "tp"), P("kv", "tp"), P("kv", "tp"))
    return jax.shard_map(device_part, mesh=mesh, in_specs=in_specs, out_specs=out_specs, check_vma=False)
```

```python
import functools

import jax
import jax.numpy as jnp
from jax import lax
from jax.experimental import pallas as pl
from jax.experimental.pallas import tpu as pltpu
from jax.sharding import PartitionSpec as P

BLOCK = 64


def tile_terms(q_tile, k_tile, v_tile, g_tile, log_total, row_dots, allowed):
    scale = q_tile.shape[-1] ** (-0.5)
    scores = (
        jnp.einsum("...qd,...kd->...qk", q_tile, k_tile, preferred_element_type=jnp.float32) * scale
    )
    probs = jnp.where(allowed, jnp.exp(scores - log_total[..., None]), 0.0)
    probs_low = probs.astype(jnp.bfloat16)
    grad_v = jnp.einsum("...qk,...qd->...kd", probs_low, g_tile, preferred_element_type=jnp.float32)
    grad_p = jnp.einsum("...qd,...kd->...qk", g_tile, v_tile, preferred_element_type=jnp.float32)
    grad_s = (probs * (grad_p - row_dots[..., None])).astype(jnp.bfloat16)
    grad_q = (
        jnp.einsum("...qk,...kd->...qd", grad_s, k_tile, preferred_element_type=jnp.float32) * scale
    )
    grad_k = (
        jnp.einsum("...qk,...qd->...kd", grad_s, q_tile, preferred_element_type=jnp.float32) * scale
    )
    return (grad_q, grad_k, grad_v)


def add_by_block(tiles, segments, block_total):
    onehot = (segments[..., None] == jnp.arange(block_total)).astype(jnp.float32)
    return jnp.einsum("hnb,hnkd->hbkd", onehot, tiles, precision=lax.Precision.HIGHEST)


def local(queries, keys, values, attended, cotangent, log_totals, block_picks, normed):
    tok_rows, row_width = queries.shape
    head_count = log_totals.shape[0]
    head_size = row_width // head_count
    local_blocks = tok_rows // BLOCK
    kv_count = lax.axis_size("kv")
    all_blocks = local_blocks * kv_count

    def by_head(matrix, blocks):
        return matrix.reshape(blocks, BLOCK, head_count, head_size).transpose(2, 0, 1, 3)

    def to_rows(tensor):
        return tensor.transpose(1, 2, 0, 3).reshape(tensor.shape[1] * BLOCK, row_width)

    q_heads = by_head(queries, local_blocks)
    k_heads = by_head(keys, local_blocks)
    v_heads = by_head(values, local_blocks)
    g_heads = by_head(cotangent, local_blocks)
    o_heads = by_head(attended, local_blocks)
    log_heads = log_totals.reshape(head_count, local_blocks, BLOCK)
    row_dots = jnp.einsum("hbqd,hbqd->hbq", g_heads, o_heads, preferred_element_type=jnp.float32)
    causal = jnp.tril(jnp.ones((BLOCK, BLOCK), bool))
    dq_diag, dk_diag, dv_diag = tile_terms(
        q_heads, k_heads, v_heads, g_heads, log_heads, row_dots, causal
    )
    q_all, g_all = (
        lax.all_gather(queries, "kv", axis=0, tiled=True),
        lax.all_gather(cotangent, "kv", axis=0, tiled=True),
    )
    log_all, dots_all = (
        lax.all_gather(log_totals, "kv", axis=1, tiled=True),
        lax.all_gather(row_dots.reshape(head_count, tok_rows), "kv", axis=1, tiled=True),
    )
    picks_all = lax.all_gather(block_picks, "kv", axis=1, tiled=True)
    most = max(2, all_blocks // 4)
    own_ids = lax.axis_index("kv") * local_blocks + jnp.arange(local_blocks)
    matched = jnp.any(picks_all[:, :, :, None] == own_ids, axis=2)
    position = jnp.cumsum(matched.astype(jnp.int32), axis=1) - 1
    slot_hit = matched[..., None] & (position[..., None] == jnp.arange(most))
    listed = jnp.sum(jnp.where(slot_hit, jnp.arange(all_blocks)[None, :, None, None], 0), axis=1)
    filled = jnp.any(slot_hit, axis=1)
    q_blocks = by_head(q_all, all_blocks)
    g_blocks = by_head(g_all, all_blocks)
    log_blocks = log_all.reshape(head_count, all_blocks, BLOCK)
    dots_blocks = dots_all.reshape(head_count, all_blocks, BLOCK)
    q_sel = jax.vmap(lambda t, i: t[i])(q_blocks, listed)
    g_sel = jax.vmap(lambda t, i: t[i])(g_blocks, listed)
    l_sel = jax.vmap(lambda t, i: t[i])(log_blocks, listed)
    d_sel = jax.vmap(lambda t, i: t[i])(dots_blocks, listed)
    tile_shape = q_sel.shape
    k_rep = jnp.broadcast_to(k_heads[:, :, None], tile_shape)
    v_rep = jnp.broadcast_to(v_heads[:, :, None], tile_shape)
    allowed = jnp.broadcast_to(filled[..., None, None], tile_shape[:4] + (BLOCK,))
    dq_sel, dk_sel, dv_sel = tile_terms(q_sel, k_rep, v_rep, g_sel, l_sel, d_sel, allowed)
    grad_k = to_rows(dk_diag + jnp.sum(dk_sel, axis=2))
    grad_v = to_rows(dv_diag + jnp.sum(dv_sel, axis=2))
    segments = jnp.where(filled, listed, all_blocks).reshape(head_count, local_blocks * most)
    dq_blocks = add_by_block(
        dq_sel.reshape(head_count, local_blocks * most, BLOCK, head_size), segments, all_blocks
    )
    dq_full = to_rows(dq_blocks)
    remote_q = lax.psum_scatter(dq_full, "kv", scatter_dimension=0, tiled=True)
    grad_queries = (remote_q + to_rows(dq_diag)).astype(jnp.bfloat16)
    full_hidden = lax.all_gather(normed, "tp", axis=1, tiled=True)
    grad_weight = lax.psum_scatter(
        lax.dot_general(
            full_hidden, grad_queries, (((0,), (0,)), ((), ())), preferred_element_type=jnp.float32
        ),
        "kv",
        scatter_dimension=0,
        tiled=True,
    )
    return (grad_queries, grad_k.astype(jnp.bfloat16), grad_v.astype(jnp.bfloat16), grad_weight)


def head_grads(q, k, v, g, log_total, row_dots, picks):
    rows = q.shape[0]
    blocks = rows // BLOCK
    scale = q.shape[-1] ** (-0.5)
    contract_last = (((1,), (1,)), ((), ()))
    contract_first = (((0,), (0,)), ((), ()))
    chosen = jnp.any(picks[:, :, None] == jnp.arange(blocks), axis=1)
    position = jnp.arange(rows)
    chosen = jnp.repeat(jnp.repeat(chosen, BLOCK, axis=0), BLOCK, axis=1)
    own = (position[:, None] // BLOCK == position[None, :] // BLOCK) & (
        position[:, None] >= position[None, :]
    )
    scores = lax.dot_general(q, k, contract_last, preferred_element_type=jnp.float32) * scale
    probs = jnp.where(chosen | own, jnp.exp(scores - log_total[:, None]), 0.0)
    grad_p = lax.dot_general(g, v, contract_last, preferred_element_type=jnp.float32)
    grad_s = (probs * (grad_p - row_dots[:, None])).astype(jnp.bfloat16)
    grad_v = lax.dot_general(
        probs.astype(jnp.bfloat16), g, contract_first, preferred_element_type=jnp.float32
    )
    grad_k = lax.dot_general(grad_s, q, contract_first, preferred_element_type=jnp.float32) * scale
    grad_q = jnp.dot(grad_s, k, preferred_element_type=jnp.float32) * scale
    return grad_q.astype(jnp.bfloat16), grad_k.astype(jnp.bfloat16), grad_v.astype(jnp.bfloat16)


def by_heads(queries, keys, values, attended, cotangent, log_totals, block_picks, normed):
    tok_rows, row_width = queries.shape
    head_count = log_totals.shape[0]
    head_size = row_width // head_count
    kv_count = lax.axis_size("kv")
    heads = head_count // kv_count
    product = cotangent.astype(jnp.float32) * attended.astype(jnp.float32)
    row_dots = jnp.sum(product.reshape(tok_rows, head_count, head_size), axis=2).T
    packed = lax.all_to_all(
        jnp.stack([queries, keys, values, cotangent]), "kv", split_axis=2, concat_axis=1, tiled=True
    )
    sides = lax.all_to_all(
        jnp.stack([log_totals, row_dots]), "kv", split_axis=1, concat_axis=2, tiled=True
    )
    picks = lax.all_to_all(block_picks, "kv", split_axis=0, concat_axis=1, tiled=True)
    features = lax.all_gather(normed, "tp", axis=1, tiled=True)
    features = lax.all_to_all(features, "kv", split_axis=1, concat_axis=0, tiled=True)
    grads = []
    for h in range(heads):
        q, k, v, g = (packed[i, :, h * head_size : (h + 1) * head_size] for i in range(4))
        grads.append(head_grads(q, k, v, g, sides[0, h], sides[1, h], picks[h]))
    dq, dk, dv = (jnp.concatenate(parts, axis=1) for parts in zip(*grads))
    dq_all = lax.all_gather(dq, "kv", axis=1, tiled=True)
    dkv = lax.all_to_all(jnp.stack([dk, dv]), "kv", split_axis=1, concat_axis=2, tiled=True)
    grad_queries = lax.dynamic_slice_in_dim(
        dq_all, lax.axis_index("kv") * tok_rows, tok_rows, axis=0
    )
    grad_weight = lax.dot_general(
        features, dq_all, (((0,), (0,)), ((), ())), preferred_element_type=jnp.float32
    )
    return (grad_queries, dkv[0], dkv[1], grad_weight)


NEVER = -1e30
LAST = (((1,), (1,)), ((), ()))
FIRST = (((0,), (0,)), ((), ()))


def mm(a, b, dims=(((1,), (0,)), ((), ()))):
    return lax.dot_general(a, b, dims, preferred_element_type=jnp.float32)


def remote(src, dst, send, recv, kv, tp):
    return pltpu.make_async_remote_copy(
        src_ref=src,
        dst_ref=dst,
        send_sem=send,
        recv_sem=recv,
        device_id=(kv, tp),
        device_id_type=pl.DeviceIdType.MESH,
    )


def one_head_kernel(
    kvs, tps, q_hbm, k_hbm, v_hbm, g_hbm, o_hbm, log_hbm, picks_hbm, n_hbm,
    gq_ref, gk_ref, gv_ref, gw_ref,
    q_ref, k_ref, v_ref, g_ref, o_ref, log_ref, picks_ref, n_ref, load,
    sent, sent_side, got, got_side, turned, plane, feats, total, dq_all, dkv, dkv_got,
    in_send, in_recv, side_send, side_recv, n1_send, n1_recv, n2_send, n2_recv,
    y_send, y_recv, core_send, core_recv,
    up_send, down_send, mate_send, line_recv, mate_recv, dkv_send, dkv_recv, inside, around,
):
    me, tp = lax.axis_index("kv"), lax.axis_index("tp")
    rows, width = q_ref.shape
    hs = width // kvs
    per = rows // BLOCK
    scale = hs ** (-0.5)
    part = feats.shape[1]

    loads = []
    pairs = ((q_hbm, q_ref), (k_hbm, k_ref), (v_hbm, v_ref), (g_hbm, g_ref), (o_hbm, o_ref))
    pairs += ((log_hbm, log_ref), (picks_hbm, picks_ref), (n_hbm, n_ref))
    for at, (source, place) in enumerate(pairs):
        loads.append(pltpu.make_async_copy(source, place, load.at[at]))
        loads[-1].start()

    barrier = pltpu.get_barrier_semaphore()
    deep = kvs // 2
    spot, side_of = me // 2, lax.rem(me, 2)
    mate = me + 1 - 2 * side_of
    opposite, partner_core = lax.rem(tp + tps // 2, tps), tp + 1 - 2 * lax.rem(tp, 2)
    outer = jnp.logical_or(spot == 0, spot == deep - 1)
    pair, second, last = spot + 1 - 2 * lax.rem(spot, 2), lax.rem(spot + 2, deep), deep - 1 - spot

    def signal(semaphore, to):
        pl.semaphore_signal(
            semaphore, inc=1, device_id=to, device_id_type=pl.DeviceIdType.MESH
        )

    def greet(semaphore):
        for to in ((mate, tp), (pair * 2 + side_of, tp), (me, opposite), (me, partner_core)):
            signal(semaphore, to)

        @pl.when(jnp.logical_not(outer))
        def _():
            signal(semaphore, (last * 2 + side_of, tp))

    touching = 5 - outer.astype(jnp.int32)
    greet(barrier)
    for copy in loads[:4]:
        copy.wait()

    for h in range(kvs):
        c = slice(h * hs, (h + 1) * hs)
        sent[h, :, : 2 * hs] = jnp.concatenate([q_ref[:, c], k_ref[:, c]], axis=1)
        sent[h, :, 2 * hs :] = jnp.concatenate([v_ref[:, c], g_ref[:, c]], axis=1)
    pl.semaphore_wait(barrier, touching)

    def main_copy(to, at):
        return remote(sent.at[to], got.at[me], in_send.at[at], in_recv.at[me], to, tp)

    def side_copy(to, at):
        return remote(
            sent_side.at[to], got_side.at[me], side_send.at[at], side_recv.at[me], to, tp
        )

    straight, crossed = side_of, 1 - side_of
    targets = [mate]
    targets += [level * 2 + s for level in (pair, second, last) for s in (straight, crossed)]
    mains = [main_copy(to, at) for at, to in enumerate(targets)]
    to_mate, to_pair, to_pair_mate, to_second, to_second_mate, to_last, to_last_mate = mains
    waits = list(mains)

    greet(inside)
    to_pair.start()

    @pl.when(jnp.logical_not(outer))
    def _():
        to_last.start()

    to_mate.start()
    for copy in loads[4:-1]:
        copy.wait()
    product = g_ref[...].astype(jnp.float32) * o_ref[...].astype(jnp.float32)
    high = product.astype(jnp.bfloat16)
    low = (product - high.astype(jnp.float32)).astype(jnp.bfloat16)
    head_of = lax.broadcasted_iota(jnp.int32, (16, width), 1) // hs
    pick = (head_of == lax.broadcasted_iota(jnp.int32, (16, width), 0)).astype(jnp.bfloat16)
    dots = mm(pick, high, LAST) + mm(pick, low, LAST)
    line = lax.broadcasted_iota(jnp.int32, (8, rows), 0)
    block_at = lax.broadcasted_iota(jnp.int32, (8, rows), 1) // BLOCK
    for h in range(kvs):
        lines = jnp.where(line == 1, dots[h : h + 1], -log_ref[h : h + 1])
        for b in range(per):
            named = picks_ref[h, b : b + 1]
            bit = jnp.where(named >= 0, jnp.left_shift(1, jnp.maximum(named, 0)), 0)
            bits = jnp.sum(bit.astype(jnp.float32), axis=1, keepdims=True)
            here_in = jnp.logical_and(line == 2, block_at == b)
            lines = jnp.where(here_in, bits, lines)
        sent_side[h] = lines
    got[me] = sent[me]
    got_side[me] = sent_side[me]
    pl.semaphore_wait(inside, touching)
    signal(around, (mate, tp))
    signal(around, (second * 2 + side_of, tp))
    to_pair_mate.start()

    @pl.when(jnp.logical_not(outer))
    def _():
        to_last_mate.start()

    to_second.start()
    pl.semaphore_wait(around, 2)

    @pl.when(outer)
    def _():
        to_last.start()
        to_last_mate.start()

    to_second_mate.start()
    for at, to in enumerate(targets):
        waits.append(side_copy(to, at))
        waits[-1].start()

    loads[-1].wait()
    for b in range(n_ref.shape[1] // 128):
        c = slice(b * 128, (b + 1) * 128)
        turned[c, :] = n_ref[:, c].astype(jnp.float32).T.astype(jnp.bfloat16)
    here = pl.ds(pl.multiple_of(me * rows, rows), rows)

    def side_rows(side):
        return pl.ds(pl.multiple_of(side * rows, rows), rows)

    def plane_rows(level):
        return pl.ds(pl.multiple_of(level * 2 * rows, 2 * rows), 2 * rows)

    def n1_copy(h, j):
        return remote(
            turned.at[pl.ds((h * tps + j) * part, part)],
            plane.at[tp, :, side_rows(side_of)],
            n1_send.at[h * tps + j],
            n1_recv.at[side_of * tps + tp],
            spot * 2 + h,
            j,
        )

    for h in range(2):
        for j in range(tps):
            mine = jnp.logical_and(side_of == h, tp == j)

            @pl.when(jnp.logical_not(mine))
            def _():
                n1_copy(h, j).start()

            @pl.when(mine)
            def _():
                place = (h * tps + j) * part
                plane[j, :, h * rows : (h + 1) * rows] = turned[place : place + part, :]

    for h in range(2):
        for j in range(tps):

            @pl.when(jnp.logical_not(jnp.logical_and(side_of == h, tp == j)))
            def _():
                remote(
                    turned.at[pl.ds(0, part)],
                    plane.at[j, :, side_rows(h)],
                    n1_send.at[0],
                    n1_recv.at[h * tps + j],
                    me,
                    tp,
                ).wait_recv()

    levels = (spot, pair, second, last)

    def level_copy(k, at):
        return remote(
            plane.at[levels[k]],
            feats.at[tp, :, plane_rows(at)],
            n2_send.at[k],
            n2_recv.at[k],
            levels[k] * 2 + side_of,
            tp,
        )

    def start_level(inner_k, outer_k):
        if inner_k == outer_k:
            level_copy(inner_k, spot).start()
        else:

            @pl.when(outer)
            def _():
                level_copy(outer_k, spot).start()

            @pl.when(jnp.logical_not(outer))
            def _():
                level_copy(inner_k, spot).start()

    start_level(3, 2)
    start_level(1, 1)
    start_level(2, 3)
    waits += [level_copy(k, spot) for k in range(1, deep)]
    feats[tp, :, plane_rows(spot)] = plane[spot]

    def chunk_copy(k, owner, own, send, recv, at, to):
        rows_of = feats.at[owner, :, plane_rows(levels[k])]
        source = plane.at[spot] if own and k == 0 else rows_of
        return remote(source, rows_of, send.at[at], recv.at[at], me, to)

    def over_y(k, owner):
        return chunk_copy(k, owner, True, y_send, y_recv, k, opposite)

    def over_core(k, owner, relayed):
        return chunk_copy(
            k, owner, not relayed, core_send, core_recv, relayed * deep + k, partner_core
        )

    def pass_chunk(k):
        if k:
            level_copy(k, levels[k]).wait_recv()
        for copy in (over_y(k, tp), over_core(k, tp, 0)):
            copy.start()

    def relay_chunk(k):
        over_y(k, opposite).wait_recv()
        over_core(k, opposite, 1).start()

    waits += [over_y(k, tp) for k in range(deep)] + [over_core(k, tp, 0) for k in range(deep)]
    waits += [over_core(k, opposite, 1) for k in range(deep)]
    pass_chunk(0)

    for d in range(1, kvs):
        src = lax.rem(me + kvs - d, kvs)
        remote(
            sent_side.at[src], got_side.at[src], side_send.at[d], side_recv.at[src], src, tp
        ).wait_recv()
        remote(sent.at[src], got.at[src], in_send.at[d], in_recv.at[src], src, tp).wait_recv()

    s_at = lax.broadcasted_iota(jnp.int32, (rows, rows), 0)
    t_at = lax.broadcasted_iota(jnp.int32, (rows, rows), 1)
    own = jnp.logical_and(s_at // BLOCK == t_at // BLOCK, s_at <= t_at)
    lines = [
        jnp.concatenate([got_side[m, r : r + 1] for m in range(kvs)], axis=1) for r in range(3)
    ]
    for i in range(kvs):
        late = (kvs - i) * rows
        q = got[i:, :, :hs].reshape(late, hs)
        g = got[i:, :, 3 * hs :].reshape(late, hs)
        k = got[i, :, hs : 2 * hs]
        v = got[i, :, 2 * hs : 3 * hs]

        minus, dots, bits = (r[:, i * rows :] for r in lines)
        bits = bits.astype(jnp.int32)
        parts = []
        for b in range(per):
            named = jnp.bitwise_and(lax.shift_right_logical(bits, i * per + b), 1) == 1
            parts.append(jnp.broadcast_to(jnp.where(named, minus, NEVER), (BLOCK, late)))
        bias = jnp.concatenate(parts, axis=0)
        first = jnp.where(own, minus[:, :rows], bias[:, :rows])
        bias = first if i == kvs - 1 else jnp.concatenate([first, bias[:, rows:]], axis=1)
        probs = jnp.exp(mm(k, q, LAST) * scale + bias)
        grad_s = (probs * (mm(v, g, LAST) - dots)).astype(jnp.bfloat16)
        grad_v = mm(probs.astype(jnp.bfloat16), g)
        grad_k = mm(grad_s, q) * scale
        dkv[i] = jnp.concatenate([grad_k, grad_v], axis=1).astype(jnp.bfloat16)
        grad_q = mm(k, grad_s, FIRST)
        if i == 0:
            total[...] = grad_q
        else:
            total[:, i * rows :] += grad_q
    dq_all[me] = (total[...] * scale).astype(jnp.bfloat16)
    dkv_got[me] = dkv[me]

    pieces = 4
    piece_rows = hs // pieces
    not_top, not_bottom = spot < deep - 1, spot > 0

    def unit_copy(unit, piece, send, recv, column, to):
        rows_of = dq_all.at[unit * 2 + column, piece * piece_rows : (piece + 1) * piece_rows]
        at = unit * pieces + piece
        return remote(rows_of, rows_of, send.at[at], recv.at[at], to, tp)

    def upward(unit, piece):
        return unit_copy(unit, piece, up_send, line_recv, side_of, me + 2)

    def downward(unit, piece):
        return unit_copy(unit, piece, down_send, line_recv, side_of, me - 2)

    def across(unit, piece):
        return unit_copy(unit, piece, mate_send, mate_recv, side_of, mate)

    for piece in range(pieces):

        @pl.when(not_top)
        def _():
            upward(spot, piece).start()

        @pl.when(not_bottom)
        def _():
            downward(spot, piece).start()

    for piece in range(pieces):
        across(spot, piece).start()

    low_half = spot < deep // 2

    def dkv_copy(to, at):
        return remote(dkv.at[to], dkv_got.at[me], dkv_send.at[at], dkv_recv.at[me], to, tp)

    def near(side):
        return dkv_copy(pair * 2 + side, 2 + side)

    def far(step, side):
        level = jnp.where(low_half, deep // 2 + step, deep // 2 - 1 - step)
        return dkv_copy(level * 2 + side, 4 + 2 * step + side)

    dkv_copy(mate, 0).start()
    waits.append(dkv_copy(mate, 0))

    @pl.when(outer)
    def _():
        for side in range(2):
            near(side).start()

    for k in range(1, deep):
        pass_chunk(k)

    for z in range(1, deep):
        for piece in range(pieces):

            @pl.when(spot >= z)
            def _():
                unit_copy(spot - z, piece, up_send, line_recv, side_of, me).wait_recv()

                @pl.when(not_top)
                def _():
                    upward(spot - z, piece).start()

                across(spot - z, piece).start()

            @pl.when(spot + z < deep)
            def _():
                unit_copy(spot + z, piece, down_send, line_recv, side_of, me).wait_recv()

                @pl.when(not_bottom)
                def _():
                    downward(spot + z, piece).start()

                across(spot + z, piece).start()

        if z == 2:
            for far_copy in [far(step, side) for step in range(deep // 2) for side in range(2)]:
                far_copy.start()
                waits.append(far_copy)

            @pl.when(jnp.logical_not(outer))
            def _():
                for side in range(2):
                    near(side).start()

            waits += [near(side) for side in range(2)]
        relay_chunk(z - 1)
    relay_chunk(deep - 1)

    for d in range(deep):
        over_core(d, partner_core, 0).wait_recv()
        over_core(d, lax.rem(partner_core + tps // 2, tps), 1).wait_recv()
    step = jnp.where(spot < deep // 2, 1, deep - 1)
    for z in range(deep):
        unit = lax.rem(spot + z * step, deep)
        for piece in range(pieces):
            unit_copy(unit, piece, mate_send, mate_recv, 1 - side_of, me).wait_recv()
        c = pl.ds(pl.multiple_of(unit * 2 * hs, 2 * hs), 2 * hs)
        pair = dq_all[pl.ds(unit * 2, 2), :, here].reshape(2 * hs, rows)
        gq_ref[:, c] = pair.astype(jnp.float32).T.astype(jnp.bfloat16)
        cols = dq_all[pl.ds(unit * 2, 2)].reshape(2 * hs, kvs * rows)
        for j in range(tps):
            gw_ref[j * part : (j + 1) * part, c] = mm(feats[j], cols, LAST)

    for d in range(1, kvs):
        src = lax.rem(me + kvs - d, kvs)
        remote(
            dkv.at[src], dkv_got.at[src], dkv_send.at[d], dkv_recv.at[src], src, tp
        ).wait_recv()
    for p in range(kvs // 2):
        c = slice(p * 2 * hs, (p + 1) * 2 * hs)
        left, right = dkv_got[2 * p], dkv_got[2 * p + 1]
        gk_ref[:, c] = jnp.concatenate([left[:, :hs], right[:, :hs]], axis=1)
        gv_ref[:, c] = jnp.concatenate([left[:, hs:], right[:, hs:]], axis=1)

    for unit in range(deep):
        for piece in range(pieces):
            across(unit, piece).wait_send()

            @pl.when(jnp.logical_and(not_top, unit <= spot))
            def _():
                upward(unit, piece).wait_send()

            @pl.when(jnp.logical_and(not_bottom, unit >= spot))
            def _():
                downward(unit, piece).wait_send()

    for copy in waits:
        copy.wait_send()
    for h in range(2):
        for j in range(tps):

            @pl.when(jnp.logical_not(jnp.logical_and(side_of == h, tp == j)))
            def _():
                n1_copy(h, j).wait_send()


def finish_kernel(count, *refs):
    sources, places, done = refs[:count], refs[count : 2 * count], refs[2 * count]
    copies = [
        pltpu.make_async_copy(source, place, done.at[at])
        for at, (source, place) in enumerate(zip(sources, places))
    ]
    for copy in copies[::-1]:
        copy.start()
    for copy in copies:
        copy.wait()


def finish(arrays):
    count = len(arrays)
    return pl.pallas_call(
        functools.partial(finish_kernel, count),
        out_shape=tuple(jax.ShapeDtypeStruct(a.shape, a.dtype) for a in arrays),
        in_specs=[pl.BlockSpec(memory_space=pltpu.VMEM)] * count,
        out_specs=(pl.BlockSpec(memory_space=pltpu.HBM),) * count,
        scratch_shapes=[pltpu.SemaphoreType.DMA((count,))],
    )(*[pltpu.with_memory_space_constraint(a, pltpu.VMEM) for a in arrays])


def one_head(queries, keys, values, attended, cotangent, log_totals, block_picks, normed):
    arrays = (queries, keys, values, cotangent, attended, log_totals, block_picks, normed)
    rows, width = queries.shape
    kvs, tps = lax.axis_size("kv"), lax.axis_size("tp")
    hs = width // kvs
    local_width = normed.shape[1]
    part = local_width // kvs
    vmem = pl.BlockSpec(memory_space=pltpu.VMEM)
    dma = pltpu.SemaphoreType.DMA
    low = jnp.bfloat16
    outs = pl.pallas_call(
        functools.partial(one_head_kernel, kvs, tps),
        out_shape=(
            pltpu.VMEM((rows, width), low),
            pltpu.VMEM((rows, width), low),
            pltpu.VMEM((rows, width), low),
            pltpu.VMEM((tps * part, width), jnp.float32),
        ),
        in_specs=[pl.BlockSpec(memory_space=pl.ANY)] * 8,
        out_specs=(vmem,) * 4,
        scratch_shapes=[pltpu.VMEM((rows, width), low)] * 5
        + [
            pltpu.VMEM(log_totals.shape, jnp.float32),
            pltpu.VMEM(block_picks.shape, jnp.int32),
            pltpu.VMEM((rows, local_width), low),
            dma((8,)),
        ]
        + [
            pltpu.VMEM((kvs, rows, 4 * hs), low),
            pltpu.VMEM((kvs, 8, rows), jnp.float32),
            pltpu.VMEM((kvs, rows, 4 * hs), low),
            pltpu.VMEM((kvs, 8, rows), jnp.float32),
            pltpu.VMEM((local_width, rows), low),
            pltpu.VMEM((kvs // 2, part, 2 * rows), low),
            pltpu.VMEM((tps, part, kvs * rows), low),
            pltpu.VMEM((hs, kvs * rows), jnp.float32),
            pltpu.VMEM((kvs, hs, kvs * rows), low),
            pltpu.VMEM((kvs, rows, 2 * hs), low),
            pltpu.VMEM((kvs, rows, 2 * hs), low),
        ]
        + [dma((kvs,))] * 6
        + [dma((kvs // 2,))] * 4
        + [dma((kvs,))] * 2
        + [dma((2 * kvs,))] * 5
        + [dma((kvs,))] * 2
        + [pltpu.SemaphoreType.REGULAR] * 2,
        compiler_params=pltpu.CompilerParams(
            collective_id=0, has_side_effects=True, vmem_limit_bytes=40 * 2**20
        ),
    )(*[pltpu.with_memory_space_constraint(a, pltpu.HBM) for a in arrays])
    return finish(outs)


def device_part(*arrays):
    heads, kvs, tps = arrays[5].shape[0], lax.axis_size("kv"), lax.axis_size("tp")
    rows, width = arrays[0].shape
    if heads == kvs and kvs == 2 * tps and tps == 4 and rows == 2 * width // heads == 128 and kvs <= 8:
        return one_head(*arrays)
    if heads % kvs == 0:
        return by_heads(*arrays)
    return local(*arrays)


def solution(mesh):
    in_specs = (
        P("kv", "tp"),
        P("kv", "tp"),
        P("kv", "tp"),
        P("kv", "tp"),
        P("kv", "tp"),
        P("tp", "kv"),
        P("tp", "kv", None),
        P("kv", "tp"),
    )
    out_specs = (P("kv", "tp"), P("kv", "tp"), P("kv", "tp"), P("kv", "tp"))
    return jax.shard_map(device_part, mesh=mesh, in_specs=in_specs, out_specs=out_specs, check_vma=False)
```

```python
import functools

import jax
import jax.numpy as jnp
from jax import lax
from jax.experimental import pallas as pl
from jax.experimental.pallas import tpu as pltpu
from jax.sharding import PartitionSpec as P

BLOCK = 64


def tile_terms(q_tile, k_tile, v_tile, g_tile, log_total, row_dots, allowed):
    scale = q_tile.shape[-1] ** (-0.5)
    scores = (
        jnp.einsum("...qd,...kd->...qk", q_tile, k_tile, preferred_element_type=jnp.float32) * scale
    )
    probs = jnp.where(allowed, jnp.exp(scores - log_total[..., None]), 0.0)
    probs_low = probs.astype(jnp.bfloat16)
    grad_v = jnp.einsum("...qk,...qd->...kd", probs_low, g_tile, preferred_element_type=jnp.float32)
    grad_p = jnp.einsum("...qd,...kd->...qk", g_tile, v_tile, preferred_element_type=jnp.float32)
    grad_s = (probs * (grad_p - row_dots[..., None])).astype(jnp.bfloat16)
    grad_q = (
        jnp.einsum("...qk,...kd->...qd", grad_s, k_tile, preferred_element_type=jnp.float32) * scale
    )
    grad_k = (
        jnp.einsum("...qk,...qd->...kd", grad_s, q_tile, preferred_element_type=jnp.float32) * scale
    )
    return (grad_q, grad_k, grad_v)


def add_by_block(tiles, segments, block_total):
    onehot = (segments[..., None] == jnp.arange(block_total)).astype(jnp.float32)
    return jnp.einsum("hnb,hnkd->hbkd", onehot, tiles, precision=lax.Precision.HIGHEST)


def local(queries, keys, values, attended, cotangent, log_totals, block_picks, normed):
    tok_rows, row_width = queries.shape
    head_count = log_totals.shape[0]
    head_size = row_width // head_count
    local_blocks = tok_rows // BLOCK
    kv_count = lax.axis_size("kv")
    all_blocks = local_blocks * kv_count

    def by_head(matrix, blocks):
        return matrix.reshape(blocks, BLOCK, head_count, head_size).transpose(2, 0, 1, 3)

    def to_rows(tensor):
        return tensor.transpose(1, 2, 0, 3).reshape(tensor.shape[1] * BLOCK, row_width)

    q_heads = by_head(queries, local_blocks)
    k_heads = by_head(keys, local_blocks)
    v_heads = by_head(values, local_blocks)
    g_heads = by_head(cotangent, local_blocks)
    o_heads = by_head(attended, local_blocks)
    log_heads = log_totals.reshape(head_count, local_blocks, BLOCK)
    row_dots = jnp.einsum("hbqd,hbqd->hbq", g_heads, o_heads, preferred_element_type=jnp.float32)
    causal = jnp.tril(jnp.ones((BLOCK, BLOCK), bool))
    dq_diag, dk_diag, dv_diag = tile_terms(
        q_heads, k_heads, v_heads, g_heads, log_heads, row_dots, causal
    )
    q_all, g_all = (
        lax.all_gather(queries, "kv", axis=0, tiled=True),
        lax.all_gather(cotangent, "kv", axis=0, tiled=True),
    )
    log_all, dots_all = (
        lax.all_gather(log_totals, "kv", axis=1, tiled=True),
        lax.all_gather(row_dots.reshape(head_count, tok_rows), "kv", axis=1, tiled=True),
    )
    picks_all = lax.all_gather(block_picks, "kv", axis=1, tiled=True)
    most = max(2, all_blocks // 4)
    own_ids = lax.axis_index("kv") * local_blocks + jnp.arange(local_blocks)
    matched = jnp.any(picks_all[:, :, :, None] == own_ids, axis=2)
    position = jnp.cumsum(matched.astype(jnp.int32), axis=1) - 1
    slot_hit = matched[..., None] & (position[..., None] == jnp.arange(most))
    listed = jnp.sum(jnp.where(slot_hit, jnp.arange(all_blocks)[None, :, None, None], 0), axis=1)
    filled = jnp.any(slot_hit, axis=1)
    q_blocks = by_head(q_all, all_blocks)
    g_blocks = by_head(g_all, all_blocks)
    log_blocks = log_all.reshape(head_count, all_blocks, BLOCK)
    dots_blocks = dots_all.reshape(head_count, all_blocks, BLOCK)
    q_sel = jax.vmap(lambda t, i: t[i])(q_blocks, listed)
    g_sel = jax.vmap(lambda t, i: t[i])(g_blocks, listed)
    l_sel = jax.vmap(lambda t, i: t[i])(log_blocks, listed)
    d_sel = jax.vmap(lambda t, i: t[i])(dots_blocks, listed)
    tile_shape = q_sel.shape
    k_rep = jnp.broadcast_to(k_heads[:, :, None], tile_shape)
    v_rep = jnp.broadcast_to(v_heads[:, :, None], tile_shape)
    allowed = jnp.broadcast_to(filled[..., None, None], tile_shape[:4] + (BLOCK,))
    dq_sel, dk_sel, dv_sel = tile_terms(q_sel, k_rep, v_rep, g_sel, l_sel, d_sel, allowed)
    grad_k = to_rows(dk_diag + jnp.sum(dk_sel, axis=2))
    grad_v = to_rows(dv_diag + jnp.sum(dv_sel, axis=2))
    segments = jnp.where(filled, listed, all_blocks).reshape(head_count, local_blocks * most)
    dq_blocks = add_by_block(
        dq_sel.reshape(head_count, local_blocks * most, BLOCK, head_size), segments, all_blocks
    )
    dq_full = to_rows(dq_blocks)
    remote_q = lax.psum_scatter(dq_full, "kv", scatter_dimension=0, tiled=True)
    grad_queries = (remote_q + to_rows(dq_diag)).astype(jnp.bfloat16)
    full_hidden = lax.all_gather(normed, "tp", axis=1, tiled=True)
    grad_weight = lax.psum_scatter(
        lax.dot_general(
            full_hidden, grad_queries, (((0,), (0,)), ((), ())), preferred_element_type=jnp.float32
        ),
        "kv",
        scatter_dimension=0,
        tiled=True,
    )
    return (grad_queries, grad_k.astype(jnp.bfloat16), grad_v.astype(jnp.bfloat16), grad_weight)


def head_grads(q, k, v, g, log_total, row_dots, picks):
    rows = q.shape[0]
    blocks = rows // BLOCK
    scale = q.shape[-1] ** (-0.5)
    contract_last = (((1,), (1,)), ((), ()))
    contract_first = (((0,), (0,)), ((), ()))
    chosen = jnp.any(picks[:, :, None] == jnp.arange(blocks), axis=1)
    position = jnp.arange(rows)
    chosen = jnp.repeat(jnp.repeat(chosen, BLOCK, axis=0), BLOCK, axis=1)
    own = (position[:, None] // BLOCK == position[None, :] // BLOCK) & (
        position[:, None] >= position[None, :]
    )
    scores = lax.dot_general(q, k, contract_last, preferred_element_type=jnp.float32) * scale
    probs = jnp.where(chosen | own, jnp.exp(scores - log_total[:, None]), 0.0)
    grad_p = lax.dot_general(g, v, contract_last, preferred_element_type=jnp.float32)
    grad_s = (probs * (grad_p - row_dots[:, None])).astype(jnp.bfloat16)
    grad_v = lax.dot_general(
        probs.astype(jnp.bfloat16), g, contract_first, preferred_element_type=jnp.float32
    )
    grad_k = lax.dot_general(grad_s, q, contract_first, preferred_element_type=jnp.float32) * scale
    grad_q = jnp.dot(grad_s, k, preferred_element_type=jnp.float32) * scale
    return grad_q.astype(jnp.bfloat16), grad_k.astype(jnp.bfloat16), grad_v.astype(jnp.bfloat16)


def by_heads(queries, keys, values, attended, cotangent, log_totals, block_picks, normed):
    tok_rows, row_width = queries.shape
    head_count = log_totals.shape[0]
    head_size = row_width // head_count
    kv_count = lax.axis_size("kv")
    heads = head_count // kv_count
    product = cotangent.astype(jnp.float32) * attended.astype(jnp.float32)
    row_dots = jnp.sum(product.reshape(tok_rows, head_count, head_size), axis=2).T
    packed = lax.all_to_all(
        jnp.stack([queries, keys, values, cotangent]), "kv", split_axis=2, concat_axis=1, tiled=True
    )
    sides = lax.all_to_all(
        jnp.stack([log_totals, row_dots]), "kv", split_axis=1, concat_axis=2, tiled=True
    )
    picks = lax.all_to_all(block_picks, "kv", split_axis=0, concat_axis=1, tiled=True)
    features = lax.all_gather(normed, "tp", axis=1, tiled=True)
    features = lax.all_to_all(features, "kv", split_axis=1, concat_axis=0, tiled=True)
    grads = []
    for h in range(heads):
        q, k, v, g = (packed[i, :, h * head_size : (h + 1) * head_size] for i in range(4))
        grads.append(head_grads(q, k, v, g, sides[0, h], sides[1, h], picks[h]))
    dq, dk, dv = (jnp.concatenate(parts, axis=1) for parts in zip(*grads))
    dq_all = lax.all_gather(dq, "kv", axis=1, tiled=True)
    dkv = lax.all_to_all(jnp.stack([dk, dv]), "kv", split_axis=1, concat_axis=2, tiled=True)
    grad_queries = lax.dynamic_slice_in_dim(
        dq_all, lax.axis_index("kv") * tok_rows, tok_rows, axis=0
    )
    grad_weight = lax.dot_general(
        features, dq_all, (((0,), (0,)), ((), ())), preferred_element_type=jnp.float32
    )
    return (grad_queries, dkv[0], dkv[1], grad_weight)


NEVER = -1e30
LAST = (((1,), (1,)), ((), ()))
FIRST = (((0,), (0,)), ((), ()))


def mm(a, b, dims=(((1,), (0,)), ((), ()))):
    return lax.dot_general(a, b, dims, preferred_element_type=jnp.float32)


def remote(src, dst, send, recv, kv, tp):
    return pltpu.make_async_remote_copy(
        src_ref=src,
        dst_ref=dst,
        send_sem=send,
        recv_sem=recv,
        device_id=(kv, tp),
        device_id_type=pl.DeviceIdType.MESH,
    )


def one_head_kernel(
    kvs, tps, q_hbm, k_hbm, v_hbm, g_hbm, o_hbm, log_hbm, picks_hbm, n_hbm,
    gq_ref, gk_ref, gv_ref, gw_ref,
    q_ref, k_ref, v_ref, g_ref, o_ref, log_ref, picks_ref, n_ref, load,
    sent, sent_side, got, got_side, turned, plane, feats, total, dq_all, dkv, dkv_got,
    in_send, in_recv, side_send, side_recv, n1_send, n1_recv, n2_send, n2_recv,
    y_send, y_recv, core_send, core_recv,
    up_send, down_send, mate_send, line_recv, mate_recv, dkv_send, dkv_recv, inside, around,
):
    me, tp = lax.axis_index("kv"), lax.axis_index("tp")
    rows, width = q_ref.shape
    hs = width // kvs
    per = rows // BLOCK
    scale = hs ** (-0.5)
    part = feats.shape[1]

    loads = []
    pairs = ((q_hbm, q_ref), (k_hbm, k_ref), (v_hbm, v_ref), (g_hbm, g_ref), (o_hbm, o_ref))
    pairs += ((log_hbm, log_ref), (picks_hbm, picks_ref), (n_hbm, n_ref))
    for at, (source, place) in enumerate(pairs):
        loads.append(pltpu.make_async_copy(source, place, load.at[at]))
        loads[-1].start()

    barrier = pltpu.get_barrier_semaphore()
    deep = kvs // 2
    spot, side_of = me // 2, lax.rem(me, 2)
    mate = me + 1 - 2 * side_of
    opposite, partner_core = lax.rem(tp + tps // 2, tps), tp + 1 - 2 * lax.rem(tp, 2)
    outer = jnp.logical_or(spot == 0, spot == deep - 1)
    pair, second, last = spot + 1 - 2 * lax.rem(spot, 2), lax.rem(spot + 2, deep), deep - 1 - spot

    def signal(semaphore, to):
        pl.semaphore_signal(
            semaphore, inc=1, device_id=to, device_id_type=pl.DeviceIdType.MESH
        )

    def greet(semaphore):
        for to in ((mate, tp), (pair * 2 + side_of, tp), (me, opposite), (me, partner_core)):
            signal(semaphore, to)

        @pl.when(jnp.logical_not(outer))
        def _():
            signal(semaphore, (last * 2 + side_of, tp))

    touching = 5 - outer.astype(jnp.int32)
    greet(barrier)
    for copy in loads[:4]:
        copy.wait()

    for h in range(kvs):
        c = slice(h * hs, (h + 1) * hs)
        sent[h, :, : 2 * hs] = jnp.concatenate([q_ref[:, c], k_ref[:, c]], axis=1)
        sent[h, :, 2 * hs :] = jnp.concatenate([v_ref[:, c], g_ref[:, c]], axis=1)
    pl.semaphore_wait(barrier, touching)

    def main_copy(to, at):
        return remote(sent.at[to], got.at[me], in_send.at[at], in_recv.at[me], to, tp)

    def side_copy(to, at):
        return remote(
            sent_side.at[to], got_side.at[me], side_send.at[at], side_recv.at[me], to, tp
        )

    straight, crossed = side_of, 1 - side_of
    targets = [mate]
    targets += [level * 2 + s for level in (pair, second, last) for s in (straight, crossed)]
    mains = [main_copy(to, at) for at, to in enumerate(targets)]
    to_mate, to_pair, to_pair_mate, to_second, to_second_mate, to_last, to_last_mate = mains
    waits = list(mains)

    greet(inside)
    to_pair.start()

    @pl.when(jnp.logical_not(outer))
    def _():
        to_last.start()

    for copy in loads[4:-1]:
        copy.wait()
    product = g_ref[...].astype(jnp.float32) * o_ref[...].astype(jnp.float32)
    high = product.astype(jnp.bfloat16)
    low = (product - high.astype(jnp.float32)).astype(jnp.bfloat16)
    head_of = lax.broadcasted_iota(jnp.int32, (16, width), 1) // hs
    pick = (head_of == lax.broadcasted_iota(jnp.int32, (16, width), 0)).astype(jnp.bfloat16)
    dots = mm(pick, high, LAST) + mm(pick, low, LAST)
    line = lax.broadcasted_iota(jnp.int32, (8, rows), 0)
    block_at = lax.broadcasted_iota(jnp.int32, (8, rows), 1) // BLOCK
    for h in range(kvs):
        lines = jnp.where(line == 1, dots[h : h + 1], -log_ref[h : h + 1])
        for b in range(per):
            named = picks_ref[h, b : b + 1]
            bit = jnp.where(named >= 0, jnp.left_shift(1, jnp.maximum(named, 0)), 0)
            bits = jnp.sum(bit.astype(jnp.float32), axis=1, keepdims=True)
            here_in = jnp.logical_and(line == 2, block_at == b)
            lines = jnp.where(here_in, bits, lines)
        sent_side[h] = lines
    got[me] = sent[me]
    got_side[me] = sent_side[me]
    pl.semaphore_wait(inside, touching)
    signal(around, (mate, tp))
    signal(around, (second * 2 + side_of, tp))
    to_second.start()
    pl.semaphore_wait(around, 2)

    @pl.when(outer)
    def _():
        to_last_mate.start()
        to_last.start()

    to_second_mate.start()

    @pl.when(jnp.logical_not(outer))
    def _():
        to_last_mate.start()

    to_pair_mate.start()
    to_mate.start()

    for at, to in enumerate(targets):
        waits.append(side_copy(to, at))
        waits[-1].start()

    loads[-1].wait()
    for b in range(n_ref.shape[1] // 128):
        c = slice(b * 128, (b + 1) * 128)
        turned[c, :] = n_ref[:, c].astype(jnp.float32).T.astype(jnp.bfloat16)
    here = pl.ds(pl.multiple_of(me * rows, rows), rows)

    def side_rows(side):
        return pl.ds(pl.multiple_of(side * rows, rows), rows)

    def plane_rows(level):
        return pl.ds(pl.multiple_of(level * 2 * rows, 2 * rows), 2 * rows)

    def n1_copy(h, j):
        return remote(
            turned.at[pl.ds((h * tps + j) * part, part)],
            plane.at[tp, :, side_rows(side_of)],
            n1_send.at[h * tps + j],
            n1_recv.at[side_of * tps + tp],
            spot * 2 + h,
            j,
        )

    for h in range(2):
        for j in range(tps):
            mine = jnp.logical_and(side_of == h, tp == j)

            @pl.when(jnp.logical_not(mine))
            def _():
                n1_copy(h, j).start()

            @pl.when(mine)
            def _():
                place = (h * tps + j) * part
                plane[j, :, h * rows : (h + 1) * rows] = turned[place : place + part, :]

    for h in range(2):
        for j in range(tps):

            @pl.when(jnp.logical_not(jnp.logical_and(side_of == h, tp == j)))
            def _():
                remote(
                    turned.at[pl.ds(0, part)],
                    plane.at[j, :, side_rows(h)],
                    n1_send.at[0],
                    n1_recv.at[h * tps + j],
                    me,
                    tp,
                ).wait_recv()

    levels = (spot, pair, second, last)

    def level_copy(k, at):
        return remote(
            plane.at[levels[k]],
            feats.at[tp, :, plane_rows(at)],
            n2_send.at[k],
            n2_recv.at[k],
            levels[k] * 2 + side_of,
            tp,
        )

    def start_level(inner_k, outer_k):
        if inner_k == outer_k:
            level_copy(inner_k, spot).start()
        else:

            @pl.when(outer)
            def _():
                level_copy(outer_k, spot).start()

            @pl.when(jnp.logical_not(outer))
            def _():
                level_copy(inner_k, spot).start()

    start_level(3, 2)
    start_level(1, 1)
    start_level(2, 3)
    waits += [level_copy(k, spot) for k in range(1, deep)]
    feats[tp, :, plane_rows(spot)] = plane[spot]

    def chunk_copy(k, owner, own, send, recv, at, to):
        rows_of = feats.at[owner, :, plane_rows(levels[k])]
        source = plane.at[spot] if own and k == 0 else rows_of
        return remote(source, rows_of, send.at[at], recv.at[at], me, to)

    def over_y(k, owner):
        return chunk_copy(k, owner, True, y_send, y_recv, k, opposite)

    def over_core(k, owner, relayed):
        return chunk_copy(
            k, owner, not relayed, core_send, core_recv, relayed * deep + k, partner_core
        )

    def pass_chunk(k):
        if k:
            level_copy(k, levels[k]).wait_recv()
        for copy in (over_y(k, tp), over_core(k, tp, 0)):
            copy.start()

    def relay_chunk(k):
        over_y(k, opposite).wait_recv()
        over_core(k, opposite, 1).start()

    waits += [over_y(k, tp) for k in range(deep)] + [over_core(k, tp, 0) for k in range(deep)]
    waits += [over_core(k, opposite, 1) for k in range(deep)]
    pass_chunk(0)

    for d in range(1, kvs):
        src = lax.rem(me + kvs - d, kvs)
        remote(
            sent_side.at[src], got_side.at[src], side_send.at[d], side_recv.at[src], src, tp
        ).wait_recv()
        remote(sent.at[src], got.at[src], in_send.at[d], in_recv.at[src], src, tp).wait_recv()

    s_at = lax.broadcasted_iota(jnp.int32, (rows, rows), 0)
    t_at = lax.broadcasted_iota(jnp.int32, (rows, rows), 1)
    own = jnp.logical_and(s_at // BLOCK == t_at // BLOCK, s_at <= t_at)
    lines = [
        jnp.concatenate([got_side[m, r : r + 1] for m in range(kvs)], axis=1) for r in range(3)
    ]
    pieces = 4
    piece_columns = kvs * rows // pieces
    not_top, not_bottom = spot < deep - 1, spot > 0

    def unit_copy(unit, piece, send, recv, column, to):
        columns = slice(piece * piece_columns, (piece + 1) * piece_columns)
        columns_of = dq_all.at[unit * 2 + column, :, columns]
        at = unit * pieces + piece
        return remote(columns_of, columns_of, send.at[at], recv.at[at], to, tp)

    def upward(unit, piece):
        return unit_copy(unit, piece, up_send, line_recv, side_of, me + 2)

    def downward(unit, piece):
        return unit_copy(unit, piece, down_send, line_recv, side_of, me - 2)

    def across(unit, piece):
        return unit_copy(unit, piece, mate_send, mate_recv, side_of, mate)

    def launch(piece):
        columns = slice(piece * piece_columns, (piece + 1) * piece_columns)
        dq_all[me, :, columns] = (total[:, columns] * scale).astype(jnp.bfloat16)

        @pl.when(not_top)
        def _():
            upward(spot, piece).start()

        @pl.when(not_bottom)
        def _():
            downward(spot, piece).start()

        across(spot, piece).start()

    for i in range(kvs):
        late = (kvs - i) * rows
        q = got[i:, :, :hs].reshape(late, hs)
        g = got[i:, :, 3 * hs :].reshape(late, hs)
        k = got[i, :, hs : 2 * hs]
        v = got[i, :, 2 * hs : 3 * hs]

        minus, dots, bits = (r[:, i * rows :] for r in lines)
        bits = bits.astype(jnp.int32)
        parts = []
        for b in range(per):
            named = jnp.bitwise_and(lax.shift_right_logical(bits, i * per + b), 1) == 1
            parts.append(jnp.broadcast_to(jnp.where(named, minus, NEVER), (BLOCK, late)))
        bias = jnp.concatenate(parts, axis=0)
        first = jnp.where(own, minus[:, :rows], bias[:, :rows])
        bias = first if i == kvs - 1 else jnp.concatenate([first, bias[:, rows:]], axis=1)
        probs = jnp.exp(mm(k, q, LAST) * scale + bias)
        grad_s = (probs * (mm(v, g, LAST) - dots)).astype(jnp.bfloat16)
        grad_v = mm(probs.astype(jnp.bfloat16), g)
        grad_k = mm(grad_s, q) * scale
        dkv[i] = jnp.concatenate([grad_k, grad_v], axis=1).astype(jnp.bfloat16)
        grad_q = mm(k, grad_s, FIRST)
        if i == 0:
            total[...] = grad_q
        else:
            total[:, i * rows :] += grad_q
        if i == 1:
            launch(0)
        if i == 3:
            launch(1)
        if i == 5:
            launch(2)
        if i == 7:
            launch(3)
    dkv_got[me] = dkv[me]

    low_half = spot < deep // 2

    def dkv_copy(to, at):
        return remote(dkv.at[to], dkv_got.at[me], dkv_send.at[at], dkv_recv.at[me], to, tp)

    def near(side):
        return dkv_copy(pair * 2 + side, 2 + side)

    def far(step, side):
        level = jnp.where(low_half, deep // 2 + step, deep // 2 - 1 - step)
        return dkv_copy(level * 2 + side, 4 + 2 * step + side)

    dkv_copy(mate, 0).start()
    waits.append(dkv_copy(mate, 0))

    @pl.when(outer)
    def _():
        for side in range(2):
            near(side).start()

    for k in range(1, deep):
        pass_chunk(k)

    for z in range(1, deep):
        for piece in range(pieces):

            @pl.when(spot >= z)
            def _():
                unit_copy(spot - z, piece, up_send, line_recv, side_of, me).wait_recv()

                @pl.when(not_top)
                def _():
                    upward(spot - z, piece).start()

                across(spot - z, piece).start()

            @pl.when(spot + z < deep)
            def _():
                unit_copy(spot + z, piece, down_send, line_recv, side_of, me).wait_recv()

                @pl.when(not_bottom)
                def _():
                    downward(spot + z, piece).start()

                across(spot + z, piece).start()

        if z == 2:
            for far_copy in [far(step, side) for step in range(deep // 2) for side in range(2)]:
                far_copy.start()
                waits.append(far_copy)

            @pl.when(jnp.logical_not(outer))
            def _():
                for side in range(2):
                    near(side).start()

            waits += [near(side) for side in range(2)]
        relay_chunk(z - 1)
    relay_chunk(deep - 1)

    for d in range(deep):
        over_core(d, partner_core, 0).wait_recv()
        over_core(d, lax.rem(partner_core + tps // 2, tps), 1).wait_recv()
    step = jnp.where(spot < deep // 2, 1, deep - 1)
    for z in range(deep):
        unit = lax.rem(spot + z * step, deep)
        for piece in range(pieces):
            unit_copy(unit, piece, mate_send, mate_recv, 1 - side_of, me).wait_recv()
        c = pl.ds(pl.multiple_of(unit * 2 * hs, 2 * hs), 2 * hs)
        pair = dq_all[pl.ds(unit * 2, 2), :, here].reshape(2 * hs, rows)
        gq_ref[:, c] = pair.astype(jnp.float32).T.astype(jnp.bfloat16)
        cols = dq_all[pl.ds(unit * 2, 2)].reshape(2 * hs, kvs * rows)
        for j in range(tps):
            gw_ref[j * part : (j + 1) * part, c] = mm(feats[j], cols, LAST)

    for d in range(1, kvs):
        src = lax.rem(me + kvs - d, kvs)
        remote(
            dkv.at[src], dkv_got.at[src], dkv_send.at[d], dkv_recv.at[src], src, tp
        ).wait_recv()
    for p in range(kvs // 2):
        c = slice(p * 2 * hs, (p + 1) * 2 * hs)
        left, right = dkv_got[2 * p], dkv_got[2 * p + 1]
        gk_ref[:, c] = jnp.concatenate([left[:, :hs], right[:, :hs]], axis=1)
        gv_ref[:, c] = jnp.concatenate([left[:, hs:], right[:, hs:]], axis=1)

    for unit in range(deep):
        for piece in range(pieces):
            across(unit, piece).wait_send()

            @pl.when(jnp.logical_and(not_top, unit <= spot))
            def _():
                upward(unit, piece).wait_send()

            @pl.when(jnp.logical_and(not_bottom, unit >= spot))
            def _():
                downward(unit, piece).wait_send()

    for copy in waits:
        copy.wait_send()
    for h in range(2):
        for j in range(tps):

            @pl.when(jnp.logical_not(jnp.logical_and(side_of == h, tp == j)))
            def _():
                n1_copy(h, j).wait_send()


def finish_kernel(count, *refs):
    sources, places, done = refs[:count], refs[count : 2 * count], refs[2 * count]
    copies = [
        pltpu.make_async_copy(source, place, done.at[at])
        for at, (source, place) in enumerate(zip(sources, places))
    ]
    for copy in copies[::-1]:
        copy.start()
    for copy in copies:
        copy.wait()


def finish(arrays):
    count = len(arrays)
    return pl.pallas_call(
        functools.partial(finish_kernel, count),
        out_shape=tuple(jax.ShapeDtypeStruct(a.shape, a.dtype) for a in arrays),
        in_specs=[pl.BlockSpec(memory_space=pltpu.VMEM)] * count,
        out_specs=(pl.BlockSpec(memory_space=pltpu.HBM),) * count,
        scratch_shapes=[pltpu.SemaphoreType.DMA((count,))],
    )(*[pltpu.with_memory_space_constraint(a, pltpu.VMEM) for a in arrays])


def one_head(queries, keys, values, attended, cotangent, log_totals, block_picks, normed):
    arrays = (queries, keys, values, cotangent, attended, log_totals, block_picks, normed)
    rows, width = queries.shape
    kvs, tps = lax.axis_size("kv"), lax.axis_size("tp")
    hs = width // kvs
    local_width = normed.shape[1]
    part = local_width // kvs
    vmem = pl.BlockSpec(memory_space=pltpu.VMEM)
    dma = pltpu.SemaphoreType.DMA
    low = jnp.bfloat16
    outs = pl.pallas_call(
        functools.partial(one_head_kernel, kvs, tps),
        out_shape=(
            pltpu.VMEM((rows, width), low),
            pltpu.VMEM((rows, width), low),
            pltpu.VMEM((rows, width), low),
            pltpu.VMEM((tps * part, width), jnp.float32),
        ),
        in_specs=[pl.BlockSpec(memory_space=pl.ANY)] * 8,
        out_specs=(vmem,) * 4,
        scratch_shapes=[pltpu.VMEM((rows, width), low)] * 5
        + [
            pltpu.VMEM(log_totals.shape, jnp.float32),
            pltpu.VMEM(block_picks.shape, jnp.int32),
            pltpu.VMEM((rows, local_width), low),
            dma((8,)),
        ]
        + [
            pltpu.VMEM((kvs, rows, 4 * hs), low),
            pltpu.VMEM((kvs, 8, rows), jnp.float32),
            pltpu.VMEM((kvs, rows, 4 * hs), low),
            pltpu.VMEM((kvs, 8, rows), jnp.float32),
            pltpu.VMEM((local_width, rows), low),
            pltpu.VMEM((kvs // 2, part, 2 * rows), low),
            pltpu.VMEM((tps, part, kvs * rows), low),
            pltpu.VMEM((hs, kvs * rows), jnp.float32),
            pltpu.VMEM((kvs, hs, kvs * rows), low),
            pltpu.VMEM((kvs, rows, 2 * hs), low),
            pltpu.VMEM((kvs, rows, 2 * hs), low),
        ]
        + [dma((kvs,))] * 6
        + [dma((kvs // 2,))] * 4
        + [dma((kvs,))] * 2
        + [dma((2 * kvs,))] * 5
        + [dma((kvs,))] * 2
        + [pltpu.SemaphoreType.REGULAR] * 2,
        compiler_params=pltpu.CompilerParams(
            collective_id=0, has_side_effects=True, vmem_limit_bytes=40 * 2**20
        ),
    )(*[pltpu.with_memory_space_constraint(a, pltpu.HBM) for a in arrays])
    return finish(outs)


def device_part(*arrays):
    heads, kvs, tps = arrays[5].shape[0], lax.axis_size("kv"), lax.axis_size("tp")
    rows, width = arrays[0].shape
    if heads == kvs and kvs == 2 * tps and tps == 4 and rows == 2 * width // heads == 128 and kvs <= 8:
        return one_head(*arrays)
    if heads % kvs == 0:
        return by_heads(*arrays)
    return local(*arrays)


def solution(mesh):
    in_specs = (
        P("kv", "tp"),
        P("kv", "tp"),
        P("kv", "tp"),
        P("kv", "tp"),
        P("kv", "tp"),
        P("tp", "kv"),
        P("tp", "kv", None),
        P("kv", "tp"),
    )
    out_specs = (P("kv", "tp"), P("kv", "tp"), P("kv", "tp"), P("kv", "tp"))
    return jax.shard_map(device_part, mesh=mesh, in_specs=in_specs, out_specs=out_specs, check_vma=False)
```

```python
import functools

import jax
import jax.numpy as jnp
from jax import lax
from jax.experimental import pallas as pl
from jax.experimental.pallas import tpu as pltpu
from jax.sharding import PartitionSpec as P

BLOCK = 64


def tile_terms(q_tile, k_tile, v_tile, g_tile, log_total, row_dots, allowed):
    scale = q_tile.shape[-1] ** (-0.5)
    scores = (
        jnp.einsum("...qd,...kd->...qk", q_tile, k_tile, preferred_element_type=jnp.float32) * scale
    )
    probs = jnp.where(allowed, jnp.exp(scores - log_total[..., None]), 0.0)
    probs_low = probs.astype(jnp.bfloat16)
    grad_v = jnp.einsum("...qk,...qd->...kd", probs_low, g_tile, preferred_element_type=jnp.float32)
    grad_p = jnp.einsum("...qd,...kd->...qk", g_tile, v_tile, preferred_element_type=jnp.float32)
    grad_s = (probs * (grad_p - row_dots[..., None])).astype(jnp.bfloat16)
    grad_q = (
        jnp.einsum("...qk,...kd->...qd", grad_s, k_tile, preferred_element_type=jnp.float32) * scale
    )
    grad_k = (
        jnp.einsum("...qk,...qd->...kd", grad_s, q_tile, preferred_element_type=jnp.float32) * scale
    )
    return (grad_q, grad_k, grad_v)


def add_by_block(tiles, segments, block_total):
    onehot = (segments[..., None] == jnp.arange(block_total)).astype(jnp.float32)
    return jnp.einsum("hnb,hnkd->hbkd", onehot, tiles, precision=lax.Precision.HIGHEST)


def local(queries, keys, values, attended, cotangent, log_totals, block_picks, normed):
    tok_rows, row_width = queries.shape
    head_count = log_totals.shape[0]
    head_size = row_width // head_count
    local_blocks = tok_rows // BLOCK
    kv_count = lax.axis_size("kv")
    all_blocks = local_blocks * kv_count

    def by_head(matrix, blocks):
        return matrix.reshape(blocks, BLOCK, head_count, head_size).transpose(2, 0, 1, 3)

    def to_rows(tensor):
        return tensor.transpose(1, 2, 0, 3).reshape(tensor.shape[1] * BLOCK, row_width)

    q_heads = by_head(queries, local_blocks)
    k_heads = by_head(keys, local_blocks)
    v_heads = by_head(values, local_blocks)
    g_heads = by_head(cotangent, local_blocks)
    o_heads = by_head(attended, local_blocks)
    log_heads = log_totals.reshape(head_count, local_blocks, BLOCK)
    row_dots = jnp.einsum("hbqd,hbqd->hbq", g_heads, o_heads, preferred_element_type=jnp.float32)
    causal = jnp.tril(jnp.ones((BLOCK, BLOCK), bool))
    dq_diag, dk_diag, dv_diag = tile_terms(
        q_heads, k_heads, v_heads, g_heads, log_heads, row_dots, causal
    )
    q_all, g_all = (
        lax.all_gather(queries, "kv", axis=0, tiled=True),
        lax.all_gather(cotangent, "kv", axis=0, tiled=True),
    )
    log_all, dots_all = (
        lax.all_gather(log_totals, "kv", axis=1, tiled=True),
        lax.all_gather(row_dots.reshape(head_count, tok_rows), "kv", axis=1, tiled=True),
    )
    picks_all = lax.all_gather(block_picks, "kv", axis=1, tiled=True)
    most = max(2, all_blocks // 4)
    own_ids = lax.axis_index("kv") * local_blocks + jnp.arange(local_blocks)
    matched = jnp.any(picks_all[:, :, :, None] == own_ids, axis=2)
    position = jnp.cumsum(matched.astype(jnp.int32), axis=1) - 1
    slot_hit = matched[..., None] & (position[..., None] == jnp.arange(most))
    listed = jnp.sum(jnp.where(slot_hit, jnp.arange(all_blocks)[None, :, None, None], 0), axis=1)
    filled = jnp.any(slot_hit, axis=1)
    q_blocks = by_head(q_all, all_blocks)
    g_blocks = by_head(g_all, all_blocks)
    log_blocks = log_all.reshape(head_count, all_blocks, BLOCK)
    dots_blocks = dots_all.reshape(head_count, all_blocks, BLOCK)
    q_sel = jax.vmap(lambda t, i: t[i])(q_blocks, listed)
    g_sel = jax.vmap(lambda t, i: t[i])(g_blocks, listed)
    l_sel = jax.vmap(lambda t, i: t[i])(log_blocks, listed)
    d_sel = jax.vmap(lambda t, i: t[i])(dots_blocks, listed)
    tile_shape = q_sel.shape
    k_rep = jnp.broadcast_to(k_heads[:, :, None], tile_shape)
    v_rep = jnp.broadcast_to(v_heads[:, :, None], tile_shape)
    allowed = jnp.broadcast_to(filled[..., None, None], tile_shape[:4] + (BLOCK,))
    dq_sel, dk_sel, dv_sel = tile_terms(q_sel, k_rep, v_rep, g_sel, l_sel, d_sel, allowed)
    grad_k = to_rows(dk_diag + jnp.sum(dk_sel, axis=2))
    grad_v = to_rows(dv_diag + jnp.sum(dv_sel, axis=2))
    segments = jnp.where(filled, listed, all_blocks).reshape(head_count, local_blocks * most)
    dq_blocks = add_by_block(
        dq_sel.reshape(head_count, local_blocks * most, BLOCK, head_size), segments, all_blocks
    )
    dq_full = to_rows(dq_blocks)
    remote_q = lax.psum_scatter(dq_full, "kv", scatter_dimension=0, tiled=True)
    grad_queries = (remote_q + to_rows(dq_diag)).astype(jnp.bfloat16)
    full_hidden = lax.all_gather(normed, "tp", axis=1, tiled=True)
    grad_weight = lax.psum_scatter(
        lax.dot_general(
            full_hidden, grad_queries, (((0,), (0,)), ((), ())), preferred_element_type=jnp.float32
        ),
        "kv",
        scatter_dimension=0,
        tiled=True,
    )
    return (grad_queries, grad_k.astype(jnp.bfloat16), grad_v.astype(jnp.bfloat16), grad_weight)


def head_grads(q, k, v, g, log_total, row_dots, picks):
    rows = q.shape[0]
    blocks = rows // BLOCK
    scale = q.shape[-1] ** (-0.5)
    contract_last = (((1,), (1,)), ((), ()))
    contract_first = (((0,), (0,)), ((), ()))
    chosen = jnp.any(picks[:, :, None] == jnp.arange(blocks), axis=1)
    position = jnp.arange(rows)
    chosen = jnp.repeat(jnp.repeat(chosen, BLOCK, axis=0), BLOCK, axis=1)
    own = (position[:, None] // BLOCK == position[None, :] // BLOCK) & (
        position[:, None] >= position[None, :]
    )
    scores = lax.dot_general(q, k, contract_last, preferred_element_type=jnp.float32) * scale
    probs = jnp.where(chosen | own, jnp.exp(scores - log_total[:, None]), 0.0)
    grad_p = lax.dot_general(g, v, contract_last, preferred_element_type=jnp.float32)
    grad_s = (probs * (grad_p - row_dots[:, None])).astype(jnp.bfloat16)
    grad_v = lax.dot_general(
        probs.astype(jnp.bfloat16), g, contract_first, preferred_element_type=jnp.float32
    )
    grad_k = lax.dot_general(grad_s, q, contract_first, preferred_element_type=jnp.float32) * scale
    grad_q = jnp.dot(grad_s, k, preferred_element_type=jnp.float32) * scale
    return grad_q.astype(jnp.bfloat16), grad_k.astype(jnp.bfloat16), grad_v.astype(jnp.bfloat16)


def by_heads(queries, keys, values, attended, cotangent, log_totals, block_picks, normed):
    tok_rows, row_width = queries.shape
    head_count = log_totals.shape[0]
    head_size = row_width // head_count
    kv_count = lax.axis_size("kv")
    heads = head_count // kv_count
    product = cotangent.astype(jnp.float32) * attended.astype(jnp.float32)
    row_dots = jnp.sum(product.reshape(tok_rows, head_count, head_size), axis=2).T
    packed = lax.all_to_all(
        jnp.stack([queries, keys, values, cotangent]), "kv", split_axis=2, concat_axis=1, tiled=True
    )
    sides = lax.all_to_all(
        jnp.stack([log_totals, row_dots]), "kv", split_axis=1, concat_axis=2, tiled=True
    )
    picks = lax.all_to_all(block_picks, "kv", split_axis=0, concat_axis=1, tiled=True)
    features = lax.all_gather(normed, "tp", axis=1, tiled=True)
    features = lax.all_to_all(features, "kv", split_axis=1, concat_axis=0, tiled=True)
    grads = []
    for h in range(heads):
        q, k, v, g = (packed[i, :, h * head_size : (h + 1) * head_size] for i in range(4))
        grads.append(head_grads(q, k, v, g, sides[0, h], sides[1, h], picks[h]))
    dq, dk, dv = (jnp.concatenate(parts, axis=1) for parts in zip(*grads))
    dq_all = lax.all_gather(dq, "kv", axis=1, tiled=True)
    dkv = lax.all_to_all(jnp.stack([dk, dv]), "kv", split_axis=1, concat_axis=2, tiled=True)
    grad_queries = lax.dynamic_slice_in_dim(
        dq_all, lax.axis_index("kv") * tok_rows, tok_rows, axis=0
    )
    grad_weight = lax.dot_general(
        features, dq_all, (((0,), (0,)), ((), ())), preferred_element_type=jnp.float32
    )
    return (grad_queries, dkv[0], dkv[1], grad_weight)


NEVER = -1e30
LAST = (((1,), (1,)), ((), ()))
FIRST = (((0,), (0,)), ((), ()))


def mm(a, b, dims=(((1,), (0,)), ((), ()))):
    return lax.dot_general(a, b, dims, preferred_element_type=jnp.float32)


def remote(src, dst, send, recv, kv, tp):
    return pltpu.make_async_remote_copy(
        src_ref=src,
        dst_ref=dst,
        send_sem=send,
        recv_sem=recv,
        device_id=(kv, tp),
        device_id_type=pl.DeviceIdType.MESH,
    )


def one_head_kernel(
    kvs, tps, q_hbm, k_hbm, v_hbm, g_hbm, o_hbm, log_hbm, picks_hbm, n_hbm,
    gq_ref, gk_ref, gv_ref, gw_ref,
    q_ref, k_ref, v_ref, g_ref, o_ref, log_ref, picks_ref, n_ref, load,
    sent, sent_side, got, got_side, turned, plane, feats, total, dq_all, dkv, dkv_got,
    in_send, in_recv, side_send, side_recv, n1_send, n1_recv, n2_send, n2_recv,
    y_send, y_recv, core_send, core_recv,
    up_send, down_send, mate_send, line_recv, mate_recv, dkv_send, dkv_recv, inside, around,
):
    me, tp = lax.axis_index("kv"), lax.axis_index("tp")
    rows, width = q_ref.shape
    hs = width // kvs
    per = rows // BLOCK
    scale = hs ** (-0.5)
    part = feats.shape[1]

    loads = []
    pairs = ((q_hbm, q_ref), (k_hbm, k_ref), (v_hbm, v_ref), (g_hbm, g_ref), (o_hbm, o_ref))
    pairs += ((log_hbm, log_ref), (picks_hbm, picks_ref), (n_hbm, n_ref))
    for at, (source, place) in enumerate(pairs):
        loads.append(pltpu.make_async_copy(source, place, load.at[at]))
        loads[-1].start()

    barrier = pltpu.get_barrier_semaphore()
    deep = kvs // 2
    spot, side_of = me // 2, lax.rem(me, 2)
    mate = me + 1 - 2 * side_of
    opposite, partner_core = lax.rem(tp + tps // 2, tps), tp + 1 - 2 * lax.rem(tp, 2)
    outer = jnp.logical_or(spot == 0, spot == deep - 1)
    pair, second, last = spot + 1 - 2 * lax.rem(spot, 2), lax.rem(spot + 2, deep), deep - 1 - spot

    def signal(semaphore, to):
        pl.semaphore_signal(
            semaphore, inc=1, device_id=to, device_id_type=pl.DeviceIdType.MESH
        )

    def greet(semaphore):
        for to in ((mate, tp), (pair * 2 + side_of, tp), (me, opposite), (me, partner_core)):
            signal(semaphore, to)

        @pl.when(jnp.logical_not(outer))
        def _():
            signal(semaphore, (last * 2 + side_of, tp))

    touching = 5 - outer.astype(jnp.int32)
    greet(barrier)
    for copy in loads[:4]:
        copy.wait()

    for h in range(kvs):
        c = slice(h * hs, (h + 1) * hs)
        sent[h, :, : 2 * hs] = jnp.concatenate([q_ref[:, c], k_ref[:, c]], axis=1)
        sent[h, :, 2 * hs :] = jnp.concatenate([v_ref[:, c], g_ref[:, c]], axis=1)
    pl.semaphore_wait(barrier, touching)

    def main_copy(to, at):
        return remote(sent.at[to], got.at[me], in_send.at[at], in_recv.at[me], to, tp)

    def side_copy(to, at):
        return remote(
            sent_side.at[to], got_side.at[me], side_send.at[at], side_recv.at[me], to, tp
        )

    straight, crossed = side_of, 1 - side_of
    targets = [mate]
    targets += [level * 2 + s for level in (pair, second, last) for s in (straight, crossed)]
    mains = [main_copy(to, at) for at, to in enumerate(targets)]
    to_mate, to_pair, to_pair_mate, to_second, to_second_mate, to_last, to_last_mate = mains
    waits = list(mains)

    greet(inside)
    to_pair.start()

    @pl.when(jnp.logical_not(outer))
    def _():
        to_last.start()

    for copy in loads[4:-1]:
        copy.wait()
    product = g_ref[...].astype(jnp.float32) * o_ref[...].astype(jnp.float32)
    high = product.astype(jnp.bfloat16)
    low = (product - high.astype(jnp.float32)).astype(jnp.bfloat16)
    head_of = lax.broadcasted_iota(jnp.int32, (16, width), 1) // hs
    pick = (head_of == lax.broadcasted_iota(jnp.int32, (16, width), 0)).astype(jnp.bfloat16)
    dots = mm(pick, high, LAST) + mm(pick, low, LAST)
    line = lax.broadcasted_iota(jnp.int32, (8, rows), 0)
    block_at = lax.broadcasted_iota(jnp.int32, (8, rows), 1) // BLOCK
    for h in range(kvs):
        lines = jnp.where(line == 1, dots[h : h + 1], -log_ref[h : h + 1])
        for b in range(per):
            named = picks_ref[h, b : b + 1]
            bit = jnp.where(named >= 0, jnp.left_shift(1, jnp.maximum(named, 0)), 0)
            bits = jnp.sum(bit.astype(jnp.float32), axis=1, keepdims=True)
            here_in = jnp.logical_and(line == 2, block_at == b)
            lines = jnp.where(here_in, bits, lines)
        sent_side[h] = lines
    got[me] = sent[me]
    got_side[me] = sent_side[me]
    pl.semaphore_wait(inside, touching)
    signal(around, (mate, tp))
    signal(around, (second * 2 + side_of, tp))
    to_second.start()
    pl.semaphore_wait(around, 2)

    @pl.when(outer)
    def _():
        to_last_mate.start()
        to_last.start()

    to_second_mate.start()

    @pl.when(jnp.logical_not(outer))
    def _():
        to_last_mate.start()

    to_pair_mate.start()
    to_mate.start()

    for at, to in enumerate(targets):
        waits.append(side_copy(to, at))
        waits[-1].start()

    loads[-1].wait()
    for b in range(n_ref.shape[1] // 128):
        c = slice(b * 128, (b + 1) * 128)
        turned[c, :] = n_ref[:, c].astype(jnp.float32).T.astype(jnp.bfloat16)
    here = pl.ds(pl.multiple_of(me * rows, rows), rows)

    def side_rows(side):
        return pl.ds(pl.multiple_of(side * rows, rows), rows)

    def plane_rows(level):
        return pl.ds(pl.multiple_of(level * 2 * rows, 2 * rows), 2 * rows)

    def n1_copy(h, j):
        return remote(
            turned.at[pl.ds((h * tps + j) * part, part)],
            plane.at[tp, :, side_rows(side_of)],
            n1_send.at[h * tps + j],
            n1_recv.at[side_of * tps + tp],
            spot * 2 + h,
            j,
        )

    for h in range(2):
        for j in range(tps):
            mine = jnp.logical_and(side_of == h, tp == j)

            @pl.when(jnp.logical_not(mine))
            def _():
                n1_copy(h, j).start()

            @pl.when(mine)
            def _():
                place = (h * tps + j) * part
                plane[j, :, h * rows : (h + 1) * rows] = turned[place : place + part, :]

    for h in range(2):
        for j in range(tps):

            @pl.when(jnp.logical_not(jnp.logical_and(side_of == h, tp == j)))
            def _():
                remote(
                    turned.at[pl.ds(0, part)],
                    plane.at[j, :, side_rows(h)],
                    n1_send.at[0],
                    n1_recv.at[h * tps + j],
                    me,
                    tp,
                ).wait_recv()

    levels = (spot, pair, second, last)

    def level_copy(k, at):
        return remote(
            plane.at[levels[k]],
            feats.at[tp, :, plane_rows(at)],
            n2_send.at[k],
            n2_recv.at[k],
            levels[k] * 2 + side_of,
            tp,
        )

    def start_level(inner_k, outer_k):
        if inner_k == outer_k:
            level_copy(inner_k, spot).start()
        else:

            @pl.when(outer)
            def _():
                level_copy(outer_k, spot).start()

            @pl.when(jnp.logical_not(outer))
            def _():
                level_copy(inner_k, spot).start()

    start_level(3, 2)
    start_level(1, 1)
    start_level(2, 3)
    waits += [level_copy(k, spot) for k in range(1, deep)]
    feats[tp, :, plane_rows(spot)] = plane[spot]

    def chunk_copy(k, owner, own, send, recv, at, to):
        rows_of = feats.at[owner, :, plane_rows(levels[k])]
        source = plane.at[spot] if own and k == 0 else rows_of
        return remote(source, rows_of, send.at[at], recv.at[at], me, to)

    def over_y(k, owner):
        return chunk_copy(k, owner, True, y_send, y_recv, k, opposite)

    def over_core(k, owner, relayed):
        return chunk_copy(
            k, owner, not relayed, core_send, core_recv, relayed * deep + k, partner_core
        )

    def pass_chunk(k):
        if k:
            level_copy(k, levels[k]).wait_recv()
        for copy in (over_y(k, tp), over_core(k, tp, 0)):
            copy.start()

    def relay_chunk(k):
        over_y(k, opposite).wait_recv()
        over_core(k, opposite, 1).start()

    waits += [over_y(k, tp) for k in range(deep)] + [over_core(k, tp, 0) for k in range(deep)]
    waits += [over_core(k, opposite, 1) for k in range(deep)]
    pass_chunk(0)

    for d in range(1, kvs):
        src = lax.rem(me + kvs - d, kvs)
        remote(
            sent_side.at[src], got_side.at[src], side_send.at[d], side_recv.at[src], src, tp
        ).wait_recv()
        remote(sent.at[src], got.at[src], in_send.at[d], in_recv.at[src], src, tp).wait_recv()

    s_at = lax.broadcasted_iota(jnp.int32, (rows, rows), 0)
    t_at = lax.broadcasted_iota(jnp.int32, (rows, rows), 1)
    own = jnp.logical_and(s_at // BLOCK == t_at // BLOCK, s_at <= t_at)
    lines = [
        jnp.concatenate([got_side[m, r : r + 1] for m in range(kvs)], axis=1) for r in range(3)
    ]
    pieces = 4
    piece_columns = kvs * rows // pieces
    not_top, not_bottom = spot < deep - 1, spot > 0

    def unit_copy(unit, piece, send, recv, column, to):
        columns = slice(piece * piece_columns, (piece + 1) * piece_columns)
        columns_of = dq_all.at[unit * 2 + column, :, columns]
        at = unit * pieces + piece
        return remote(columns_of, columns_of, send.at[at], recv.at[at], to, tp)

    def upward(unit, piece):
        return unit_copy(unit, piece, up_send, line_recv, side_of, me + 2)

    def downward(unit, piece):
        return unit_copy(unit, piece, down_send, line_recv, side_of, me - 2)

    def across(unit, piece):
        return unit_copy(unit, piece, mate_send, mate_recv, side_of, mate)

    def launch(piece):
        columns = slice(piece * piece_columns, (piece + 1) * piece_columns)
        dq_all[me, :, columns] = (total[:, columns] * scale).astype(jnp.bfloat16)

        @pl.when(not_top)
        def _():
            upward(spot, piece).start()

        @pl.when(not_bottom)
        def _():
            downward(spot, piece).start()

        across(spot, piece).start()

    for i in range(kvs):
        late = (kvs - i) * rows
        q = got[i:, :, :hs].reshape(late, hs)
        g = got[i:, :, 3 * hs :].reshape(late, hs)
        k = got[i, :, hs : 2 * hs]
        v = got[i, :, 2 * hs : 3 * hs]

        minus, dots, bits = (r[:, i * rows :] for r in lines)
        bits = bits.astype(jnp.int32)
        parts = []
        for b in range(per):
            named = jnp.bitwise_and(lax.shift_right_logical(bits, i * per + b), 1) == 1
            parts.append(jnp.broadcast_to(jnp.where(named, minus, NEVER), (BLOCK, late)))
        bias = jnp.concatenate(parts, axis=0)
        first = jnp.where(own, minus[:, :rows], bias[:, :rows])
        bias = first if i == kvs - 1 else jnp.concatenate([first, bias[:, rows:]], axis=1)
        probs = jnp.exp(mm(k, q, LAST) * scale + bias)
        grad_s = (probs * (mm(v, g, LAST) - dots)).astype(jnp.bfloat16)
        grad_v = mm(probs.astype(jnp.bfloat16), g)
        grad_k = mm(grad_s, q) * scale
        dkv[i] = jnp.concatenate([grad_k, grad_v], axis=1).astype(jnp.bfloat16)
        grad_q = mm(k, grad_s, FIRST)
        if i == 0:
            total[...] = grad_q
        else:
            total[:, i * rows :] += grad_q
        if i == 1:
            launch(0)
        if i == 3:
            launch(1)
        if i == 5:
            launch(2)
        if i == 7:
            launch(3)
    dkv_got[me] = dkv[me]

    low_half = spot < deep // 2

    def dkv_copy(to, at):
        return remote(dkv.at[to], dkv_got.at[me], dkv_send.at[at], dkv_recv.at[me], to, tp)

    def near(side):
        return dkv_copy(pair * 2 + side, 2 + side)

    def far(step, side):
        level = jnp.where(low_half, deep // 2 + step, deep // 2 - 1 - step)
        return dkv_copy(level * 2 + side, 4 + 2 * step + side)

    dkv_copy(mate, 0).start()
    waits.append(dkv_copy(mate, 0))

    @pl.when(outer)
    def _():
        for side in range(2):
            near(side).start()

    for k in range(1, deep):
        pass_chunk(k)

    for z in range(1, deep):
        for piece in range(pieces):

            @pl.when(spot >= z)
            def _():
                unit_copy(spot - z, piece, up_send, line_recv, side_of, me).wait_recv()

                @pl.when(not_top)
                def _():
                    upward(spot - z, piece).start()

                across(spot - z, piece).start()

            @pl.when(spot + z < deep)
            def _():
                unit_copy(spot + z, piece, down_send, line_recv, side_of, me).wait_recv()

                @pl.when(not_bottom)
                def _():
                    downward(spot + z, piece).start()

                across(spot + z, piece).start()

        if z == 2:
            for far_copy in [far(step, side) for step in range(deep // 2) for side in range(2)]:
                far_copy.start()
                waits.append(far_copy)

            @pl.when(jnp.logical_not(outer))
            def _():
                for side in range(2):
                    near(side).start()

            waits += [near(side) for side in range(2)]
        relay_chunk(z - 1)
    relay_chunk(deep - 1)

    for d in range(deep):
        over_core(d, partner_core, 0).wait_recv()
        over_core(d, lax.rem(partner_core + tps // 2, tps), 1).wait_recv()
    step = jnp.where(spot < deep // 2, 1, deep - 1)
    for z in range(deep):
        if z == deep - 1:
            for d in range(1, kvs):
                src = lax.rem(me + kvs - d, kvs)
                remote(
                    dkv.at[src], dkv_got.at[src], dkv_send.at[d], dkv_recv.at[src], src, tp
                ).wait_recv()
            for p in range(kvs // 2):
                c = slice(p * 2 * hs, (p + 1) * 2 * hs)
                left, right = dkv_got[2 * p], dkv_got[2 * p + 1]
                gk_ref[:, c] = jnp.concatenate([left[:, :hs], right[:, :hs]], axis=1)
                gv_ref[:, c] = jnp.concatenate([left[:, hs:], right[:, hs:]], axis=1)

        unit = lax.rem(spot + z * step, deep)
        for piece in range(pieces):
            unit_copy(unit, piece, mate_send, mate_recv, 1 - side_of, me).wait_recv()
        c = pl.ds(pl.multiple_of(unit * 2 * hs, 2 * hs), 2 * hs)
        pair = dq_all[pl.ds(unit * 2, 2), :, here].reshape(2 * hs, rows)
        gq_ref[:, c] = pair.astype(jnp.float32).T.astype(jnp.bfloat16)
        cols = dq_all[pl.ds(unit * 2, 2)].reshape(2 * hs, kvs * rows)
        for j in range(tps):
            gw_ref[j * part : (j + 1) * part, c] = mm(feats[j], cols, LAST)

    for unit in range(deep):
        for piece in range(pieces):
            across(unit, piece).wait_send()

            @pl.when(jnp.logical_and(not_top, unit <= spot))
            def _():
                upward(unit, piece).wait_send()

            @pl.when(jnp.logical_and(not_bottom, unit >= spot))
            def _():
                downward(unit, piece).wait_send()

    for copy in waits:
        copy.wait_send()
    for h in range(2):
        for j in range(tps):

            @pl.when(jnp.logical_not(jnp.logical_and(side_of == h, tp == j)))
            def _():
                n1_copy(h, j).wait_send()


def finish_kernel(count, *refs):
    sources, places, done = refs[:count], refs[count : 2 * count], refs[2 * count]
    copies = [
        pltpu.make_async_copy(source, place, done.at[at])
        for at, (source, place) in enumerate(zip(sources, places))
    ]
    for copy in copies[::-1]:
        copy.start()
    for copy in copies:
        copy.wait()


def finish(arrays):
    count = len(arrays)
    return pl.pallas_call(
        functools.partial(finish_kernel, count),
        out_shape=tuple(jax.ShapeDtypeStruct(a.shape, a.dtype) for a in arrays),
        in_specs=[pl.BlockSpec(memory_space=pltpu.VMEM)] * count,
        out_specs=(pl.BlockSpec(memory_space=pltpu.HBM),) * count,
        scratch_shapes=[pltpu.SemaphoreType.DMA((count,))],
    )(*[pltpu.with_memory_space_constraint(a, pltpu.VMEM) for a in arrays])


def one_head(queries, keys, values, attended, cotangent, log_totals, block_picks, normed):
    arrays = (queries, keys, values, cotangent, attended, log_totals, block_picks, normed)
    rows, width = queries.shape
    kvs, tps = lax.axis_size("kv"), lax.axis_size("tp")
    hs = width // kvs
    local_width = normed.shape[1]
    part = local_width // kvs
    vmem = pl.BlockSpec(memory_space=pltpu.VMEM)
    dma = pltpu.SemaphoreType.DMA
    low = jnp.bfloat16
    outs = pl.pallas_call(
        functools.partial(one_head_kernel, kvs, tps),
        out_shape=(
            pltpu.VMEM((rows, width), low),
            pltpu.VMEM((rows, width), low),
            pltpu.VMEM((rows, width), low),
            pltpu.VMEM((tps * part, width), jnp.float32),
        ),
        in_specs=[pl.BlockSpec(memory_space=pl.ANY)] * 8,
        out_specs=(vmem,) * 4,
        scratch_shapes=[pltpu.VMEM((rows, width), low)] * 5
        + [
            pltpu.VMEM(log_totals.shape, jnp.float32),
            pltpu.VMEM(block_picks.shape, jnp.int32),
            pltpu.VMEM((rows, local_width), low),
            dma((8,)),
        ]
        + [
            pltpu.VMEM((kvs, rows, 4 * hs), low),
            pltpu.VMEM((kvs, 8, rows), jnp.float32),
            pltpu.VMEM((kvs, rows, 4 * hs), low),
            pltpu.VMEM((kvs, 8, rows), jnp.float32),
            pltpu.VMEM((local_width, rows), low),
            pltpu.VMEM((kvs // 2, part, 2 * rows), low),
            pltpu.VMEM((tps, part, kvs * rows), low),
            pltpu.VMEM((hs, kvs * rows), jnp.float32),
            pltpu.VMEM((kvs, hs, kvs * rows), low),
            pltpu.VMEM((kvs, rows, 2 * hs), low),
            pltpu.VMEM((kvs, rows, 2 * hs), low),
        ]
        + [dma((kvs,))] * 6
        + [dma((kvs // 2,))] * 4
        + [dma((kvs,))] * 2
        + [dma((2 * kvs,))] * 5
        + [dma((kvs,))] * 2
        + [pltpu.SemaphoreType.REGULAR] * 2,
        compiler_params=pltpu.CompilerParams(
            collective_id=0, has_side_effects=True, vmem_limit_bytes=40 * 2**20
        ),
    )(*[pltpu.with_memory_space_constraint(a, pltpu.HBM) for a in arrays])
    return finish(outs)


def device_part(*arrays):
    heads, kvs, tps = arrays[5].shape[0], lax.axis_size("kv"), lax.axis_size("tp")
    rows, width = arrays[0].shape
    if heads == kvs and kvs == 2 * tps and tps == 4 and rows == 2 * width // heads == 128 and kvs <= 8:
        return one_head(*arrays)
    if heads % kvs == 0:
        return by_heads(*arrays)
    return local(*arrays)


def solution(mesh):
    in_specs = (
        P("kv", "tp"),
        P("kv", "tp"),
        P("kv", "tp"),
        P("kv", "tp"),
        P("kv", "tp"),
        P("tp", "kv"),
        P("tp", "kv", None),
        P("kv", "tp"),
    )
    out_specs = (P("kv", "tp"), P("kv", "tp"), P("kv", "tp"), P("kv", "tp"))
    return jax.shard_map(device_part, mesh=mesh, in_specs=in_specs, out_specs=out_specs, check_vma=False)
```
